512 devices in a mesh: sp: 64 (over z, y), tp: 8 (over x, core).
Axes of the slice: x: 4, y: 8, z: 8, core: 2. Of those that a mesh axis runs over, the one named last changes fastest.
Arguments:
- target: bfloat16 [16384, 2048], P(('sp', 'tp')), may hold values from -6 to 6
- source: bfloat16 [16384, 2048], P(('sp', 'tp')), may hold values from -6 to 6
- target_gain: float32 [2, 2048], replicated, may hold values from 0.1 to 1.9
- source_gain: float32 [2, 2048], replicated, may hold values from 0.1 to 1.9
- query_gain: float32 [2, 64], replicated, may hold values from 0.75 to 2.75
- key_gain: float32 [2, 64], replicated, may hold values from 0.75 to 2.75
- query_weight: bfloat16 [2, 2048, 512], P(None, None, 'tp'), may hold values from -0.125 to 0.125
- key_weight: bfloat16 [2, 2048, 128], replicated, may hold values from -0.125 to 0.125
- value_weight: bfloat16 [2, 2048, 128], replicated, may hold values from -0.125 to 0.125
- out_weight: bfloat16 [2, 512, 2048], P(None, 'tp'), may hold values from -0.25 to 0.25
Outputs:
- decoded: bfloat16 [16384, 2048], P(('sp', 'tp'))
The draws below stay inside these ranges and needn't reach their ends.
All inputs are finite; a program needn't handle non-finite values.
Results may differ from the reference program's by a relative error of at most 0.014.
Values may be sent and summed in bfloat16 or wider, within the bound.
No kernel may reach another device: no remote copies, remote signals or barrier semaphores. Data moves between devices by JAX's collectives and lax.ppermute only.
A program may use at most 64 MiB of HBM per device.

```python
import math
import jax
import jax.numpy as jnp
from jax import lax

MODEL_WIDTH = 2048
HEAD_SIZE = 64
QUERY_HEADS = 8
KEY_HEADS = 2
LAYERS = 2
SOURCE_LEN = 16384
TARGET_LEN = 16384


def block_scale(own_key, dims, pieces, smallest, top_value):
    gain, own = 1.0, jax.random.fold_in(own_key, 6)
    for position, parts in pieces:
        draws = jnp.exp(jax.random.uniform(jax.random.fold_in(own, position), (parts,), jnp.float32, smallest / len(pieces), top_value / len(pieces)))
        gain = gain * jnp.repeat(draws, dims[position] // parts).reshape([-1 if axis == position else 1 for axis in range(len(dims))])
    return gain


def noise(stream_key, shape, spread, limit, cuts=(), kind=jnp.bfloat16):
    drawn = spread * jax.random.normal(stream_key, shape, jnp.float32)
    if cuts:
        drawn = drawn * block_scale(stream_key, shape, cuts, -0.22, 0.18)
    return jnp.clip(drawn, -limit, limit).astype(kind)


def setup_inputs(seed: int = 0) -> dict:
    key_of = jax.random.split(jax.random.key(seed), 11)
    target = noise(key_of[0], (TARGET_LEN, MODEL_WIDTH), 1.0, 6.0, ((0, 512),))
    source = noise(key_of[1], (SOURCE_LEN, MODEL_WIDTH), 1.0, 6.0, ((0, 512),))
    target_gain = jnp.clip(1.0 + 0.18 * jax.random.normal(key_of[2], (LAYERS, MODEL_WIDTH), jnp.float32), 0.1, 1.9)
    source_gain = jnp.clip(1.0 + 0.18 * jax.random.normal(key_of[3], (LAYERS, MODEL_WIDTH), jnp.float32), 0.1, 1.9)
    query_gain = jnp.clip(jnp.exp(jax.random.uniform(key_of[4], (LAYERS, HEAD_SIZE), jnp.float32, math.log(0.75), math.log(2.75))), 0.75, 2.75)
    key_gain = jnp.clip(jnp.exp(jax.random.uniform(key_of[5], (LAYERS, HEAD_SIZE), jnp.float32, math.log(0.75), math.log(2.75))), 0.75, 2.75)
    query_weight = noise(key_of[6], (LAYERS, MODEL_WIDTH, QUERY_HEADS * HEAD_SIZE), MODEL_WIDTH ** -0.5, 0.125, ((2, 8),))
    key_weight = noise(key_of[7], (LAYERS, MODEL_WIDTH, KEY_HEADS * HEAD_SIZE), MODEL_WIDTH ** -0.5, 0.125)
    value_weight = noise(key_of[8], (LAYERS, MODEL_WIDTH, KEY_HEADS * HEAD_SIZE), MODEL_WIDTH ** -0.5, 0.125)
    out_weight = noise(key_of[9], (LAYERS, QUERY_HEADS * HEAD_SIZE, MODEL_WIDTH), (QUERY_HEADS * HEAD_SIZE) ** -0.5, 0.25, ((1, 8),))
    return {"target": target, "source": source, "target_gain": target_gain, "source_gain": source_gain, "query_gain": query_gain, "key_gain": key_gain, "query_weight": query_weight, "key_weight": key_weight, "value_weight": value_weight, "out_weight": out_weight}


epsilon = 1e-06

def row_norm(values, gain_row):
    inverse = lax.rsqrt(lax.optimization_barrier(jnp.mean(values * values, axis=-1, keepdims=True)) + epsilon)
    return values * inverse * gain_row

def reference(target, source, target_gain, source_gain, query_gain, key_gain, query_weight, key_weight, value_weight, out_weight):
    group_size = QUERY_HEADS // KEY_HEADS
    source_float = source.astype(jnp.float32)
    hidden = target
    block_rows = math.gcd(TARGET_LEN, 256)
    for layer_index in range(LAYERS):
        normed_source = row_norm(source_float, source_gain[layer_index]).astype(jnp.bfloat16)
        key_rows = jnp.dot(normed_source, key_weight[layer_index], preferred_element_type=jnp.float32)
        key_rows = row_norm(key_rows.reshape(SOURCE_LEN, KEY_HEADS, HEAD_SIZE), key_gain[layer_index]).astype(jnp.bfloat16)
        key_rows = lax.optimization_barrier(key_rows).astype(jnp.float32)
        value_rows = jnp.dot(normed_source, value_weight[layer_index], preferred_element_type=jnp.float32).astype(jnp.bfloat16)
        value_rows = lax.optimization_barrier(value_rows).astype(jnp.float32).reshape(SOURCE_LEN, KEY_HEADS, HEAD_SIZE)
        hidden_float = hidden.astype(jnp.float32)
        normed = row_norm(hidden_float, target_gain[layer_index]).astype(jnp.bfloat16)
        projected = jnp.dot(normed, query_weight[layer_index], preferred_element_type=jnp.float32)
        queries = row_norm(projected.reshape(TARGET_LEN, QUERY_HEADS, HEAD_SIZE), query_gain[layer_index]).astype(jnp.bfloat16)
        queries = lax.optimization_barrier(queries).astype(jnp.float32)
        queries = queries.reshape(TARGET_LEN // block_rows, block_rows, KEY_HEADS, group_size, HEAD_SIZE)

        def attend(query_block):
            scores = jnp.einsum('bkgd,skd->bkgs', query_block, key_rows) * HEAD_SIZE ** (-0.5)
            weights = jnp.exp(scores)
            rounded = lax.optimization_barrier(weights.astype(jnp.bfloat16)).astype(jnp.float32)
            weighted = jnp.einsum('bkgs,skd->bkgd', rounded, value_rows)
            total_mass = lax.optimization_barrier(jnp.sum(weights, axis=3))
            return (weighted / total_mass[..., None]).astype(jnp.bfloat16)
        attended = lax.map(attend, queries).reshape(TARGET_LEN, QUERY_HEADS * HEAD_SIZE)
        branch = jnp.dot(attended, out_weight[layer_index], preferred_element_type=jnp.float32)
        hidden = (hidden_float + branch).astype(jnp.bfloat16)
    return hidden
```

```python
import functools

import jax
import jax.numpy as jnp
from jax import lax
from jax.experimental import pallas as pl
from jax.experimental.pallas import tpu as pltpu
from jax.sharding import Mesh
from jax.sharding import PartitionSpec as P

ROWS = ("z", "y")
TP = ("x", "c")
ALL = ("z", "y", "x", "c")
EPS = 1e-06
LOG2E = 1.4426950408889634
F32 = jnp.float32
BF16 = jnp.bfloat16


def dot(a, b):
    return jnp.dot(a, b, preferred_element_type=F32)


def dot_t(a, b):
    return lax.dot_general(a, b, (((1,), (1,)), ((), ())), preferred_element_type=F32)


def rms(value):
    return lax.rsqrt(jnp.mean(value * value, axis=-1, keepdims=True) + EPS)


def head_norm(value, gain_row, head):
    rows, width = value.shape
    low = lax.broadcasted_iota(jnp.int32, (rows, 2 * head), 1) < head
    groups = []
    for start in range(0, width, 2 * head):
        part = value[:, start : start + 2 * head]
        square = part * part
        first = jnp.sum(jnp.where(low, square, 0.0), axis=-1, keepdims=True)
        second = jnp.sum(jnp.where(low, 0.0, square), axis=-1, keepdims=True)
        scale = lax.rsqrt(jnp.where(low, first, second) / head + EPS)
        groups.append(part * scale * gain_row)
    return groups


def doubled(row):
    return jnp.concatenate([row, row], axis=-1)


def source_kernel(source, gain, key_gain, key_weight, value_weight, out):
    layers, head = key_gain.shape
    value = source[...].astype(F32)
    scaled = value * rms(value)
    width = key_weight.shape[2]
    for layer in range(layers):
        normed = (scaled * gain[layer : layer + 1, :]).astype(BF16)
        keys = dot(normed, key_weight[layer])
        row = doubled(key_gain[layer : layer + 1, :])
        groups = head_norm(keys, row, head)
        for k, group in enumerate(groups):
            out[layer, :, k * 2 * head : (k + 1) * 2 * head] = group.astype(BF16)
        out[layer, :, width:] = dot(normed, value_weight[layer]).astype(BF16)


def project(normed, mine, other, row, head, core):
    own = head_norm(dot_t(normed, mine), row, head)
    far = head_norm(dot_t(normed, other), row, head)
    first = [jnp.where(core == 0, a, b) for a, b in zip(own, far)]
    second = [jnp.where(core == 0, b, a) for a, b in zip(own, far)]
    return first + second


def store_groups(out, groups, width):
    for k, group in enumerate(groups):
        out[:, k * width : (k + 1) * width] = group.astype(BF16)


def query_kernel(layer, core_ref, target, gain, query_gain, mine, other, out):
    head = query_gain.shape[1]
    value = target[...].astype(F32)
    normed = (value * rms(value) * gain[layer : layer + 1, :]).astype(BF16)
    row = doubled(query_gain[layer : layer + 1, :])
    store_groups(out, project(normed, mine[...], other[...], row, head, core_ref[0]), 2 * head)


def attended_halves(arrived, heads, head):
    total = arrived[0].astype(F32)
    for k in range(1, arrived.shape[0]):
        total = total + arrived[k].astype(F32)
    rows = total.shape[0]
    width = heads * head
    mass = total[:, width : width + heads] + total[:, width + heads : width + 2 * heads]
    low = lax.broadcasted_iota(jnp.int32, (rows, 2 * head), 1) < head
    groups = []
    for g in range(heads // 2):
        below = jnp.where(low, mass[:, 2 * g : 2 * g + 1], mass[:, 2 * g + 1 : 2 * g + 2])
        groups.append((total[:, 2 * g * head : 2 * (g + 1) * head] / below).astype(BF16))
    half = len(groups) // 2
    return jnp.concatenate(groups[:half], axis=1), jnp.concatenate(groups[half:], axis=1)


def mixed(core, arrived, hidden, mine, other, heads, head):
    even, odd = attended_halves(arrived, heads, head)
    own = jnp.where(core == 0, even, odd)
    far = jnp.where(core == 0, odd, even)
    branch = dot(own, mine[...]) + dot(far, other[...])
    return (hidden[...].astype(F32) + branch).astype(BF16)


def middle_kernel(layer, heads, core_ref, arrived, hidden, gain, query_gain, out_mine, out_other, mine, other, hidden_out, out):
    head = query_gain.shape[1]
    core = core_ref[0]
    now = mixed(core, arrived, hidden, out_mine, out_other, heads, head)
    hidden_out[...] = now
    value = now.astype(F32)
    normed = (value * rms(value) * gain[layer : layer + 1, :]).astype(BF16)
    row = doubled(query_gain[layer : layer + 1, :])
    store_groups(out, project(normed, mine[...], other[...], row, head, core), 2 * head)


def last_kernel(heads, head, core_ref, arrived, hidden, out_mine, out_other, hidden_out):
    hidden_out[...] = mixed(core_ref[0], arrived, hidden, out_mine, out_other, heads, head)


def attention_kernel(heads, head, tile, queries, pairs, out, rhs, value_t, gathered):
    keys = pairs.shape[0]
    width = 2 * head
    columns = queries.shape[0]
    factor = LOG2E * head**-0.5
    turned = jnp.transpose(queries[...].astype(F32)).astype(BF16)
    zero = jnp.zeros((head, columns), BF16)
    per = heads // 4
    for p in range(heads):
        kv = (p % 4) // 2
        rhs[p, kv * head : (kv + 1) * head, :] = turned[p * head : (p + 1) * head, :]
        rhs[p, (1 - kv) * head : (2 - kv) * head, :] = zero
    value_t[...] = jnp.transpose(pairs[:, width:].astype(F32)).astype(BF16)
    for kv in range(2):

        def one_head(j, carry, kv=kv):
            p = (j // 2) * 4 + 2 * kv + j % 2
            right = rhs[p]
            mass = jnp.zeros((8, columns), F32)
            total = None
            for t in range(keys // tile):
                score = dot(pairs[t * tile : (t + 1) * tile, :width], right)
                weight = jnp.exp2(score * factor)
                mass = mass + jnp.sum(weight.reshape(tile // 8, 8, columns), axis=0)
                part = dot(value_t[:, t * tile : (t + 1) * tile], weight.astype(BF16))
                total = part if total is None else total + part
            gathered[pl.ds(pl.multiple_of(p * head, head), head), :] = total[kv * head : (kv + 1) * head, :]
            mass = jnp.sum(mass, axis=0, keepdims=True)
            top = mass.astype(BF16).astype(F32)
            gathered[pl.ds(heads * head + p, 1), :] = top
            gathered[pl.ds(heads * head + heads + p, 1), :] = mass - top
            return carry

        lax.fori_loop(0, 2 * per, one_head, 0)
    rest = heads * head + 2 * heads
    gathered[rest:, :] = jnp.zeros((gathered.shape[0] - rest, columns), F32)
    out[...] = jnp.transpose(gathered[...]).astype(BF16)


def call(kernel, shapes, scratch=(), flops=1000000, prefetch=0):
    one = not isinstance(shapes, (list, tuple))
    specs = pl.BlockSpec(memory_space=pltpu.VMEM)
    return pl.pallas_call(
        kernel,
        out_shape=shapes,
        out_specs=specs if one else [specs] * len(shapes),
        scratch_shapes=list(scratch),
        compiler_params=pltpu.CompilerParams(vmem_limit_bytes=40 * 1024 * 1024),
        cost_estimate=pl.CostEstimate(flops=flops, bytes_accessed=1000000, transcendentals=0),
    )


def with_core(kernel, shapes, count, flops):
    one = not isinstance(shapes, (list, tuple))
    spec = pl.BlockSpec(memory_space=pltpu.VMEM)
    return pl.pallas_call(
        kernel,
        out_shape=shapes,
        in_specs=[pl.BlockSpec(memory_space=pltpu.SMEM)] + [spec] * count,
        out_specs=spec if one else [spec] * len(shapes),
        compiler_params=pltpu.CompilerParams(vmem_limit_bytes=40 * 1024 * 1024),
        cost_estimate=pl.CostEstimate(flops=flops, bytes_accessed=1000000, transcendentals=0),
    )


def to_all(value, axis):
    copies = jnp.broadcast_to(value, (lax.axis_size(axis), *value.shape))
    return lax.all_to_all(copies, axis, split_axis=0, concat_axis=0, tiled=True)


def body(target, source, target_gain, source_gain, query_gain, key_gain, query_weight, key_weight, value_weight, out_weight):
    layers, _, head_columns = query_weight.shape
    head = query_gain.shape[1]
    heads = head_columns // head * lax.axis_size(TP)
    rows, model = target.shape
    group = rows * lax.axis_size(TP)
    shapes = jax.ShapeDtypeStruct
    core = lax.axis_index("c").reshape(1)

    query_t = jnp.swapaxes(query_weight, 1, 2)

    def full(piece):
        mine = to_all(piece, "x").reshape(-1, model)
        other = lax.ppermute(mine, "c", [(0, 1), (1, 0)])
        return mine, other

    pairs = call(source_kernel, shapes((layers, rows, 2 * key_weight.shape[2]), BF16), flops=200000000)(
        source, source_gain, key_gain, key_weight, value_weight
    )
    query_full = [full(query_t[0])]
    arrived_pairs = [to_all(pairs[0], ROWS)]
    out_full = [full(out_weight[0])]
    query_full.append(full(query_t[1]))
    arrived_pairs.append(to_all(pairs[1], ROWS))
    out_full.append(full(out_weight[1]))

    width = heads * head
    wide = width + 128
    queries = with_core(functools.partial(query_kernel, 0), shapes((rows, width), BF16), 5, 200000000)(
        core, target, target_gain, query_gain, *query_full[0]
    )
    hidden = target
    for layer in range(layers):
        everyone = to_all(queries, TP).reshape(group, width)
        kv = arrived_pairs[layer].reshape(-1, 4 * head)
        partial = call(
            functools.partial(attention_kernel, heads, head, 256),
            shapes((group, wide), BF16),
            scratch=[
                pltpu.VMEM((heads, 2 * head, group), BF16),
                pltpu.VMEM((2 * head, kv.shape[0]), BF16),
                pltpu.VMEM((wide, group), F32),
            ],
            flops=5000000000,
        )(everyone, kv)
        arrived = lax.all_to_all(partial.reshape(-1, rows, wide), TP, split_axis=0, concat_axis=0, tiled=True)
        if layer + 1 < layers:
            hidden, queries = with_core(
                functools.partial(middle_kernel, layer + 1, heads),
                [shapes((rows, model), BF16), shapes((rows, width), BF16)],
                8,
                400000000,
            )(core, arrived, hidden, target_gain, query_gain, *out_full[layer], *query_full[layer + 1])
        else:
            hidden = with_core(functools.partial(last_kernel, heads, head), shapes((rows, model), BF16), 4, 200000000)(
                core, arrived, hidden, *out_full[layer]
            )
    return hidden


def solution(mesh):
    columns = mesh.shape["tp"]
    split = Mesh(mesh.devices.reshape(8, 8, columns // 2, 2), ALL)
    return jax.shard_map(
        body,
        mesh=split,
        in_specs=(P(ALL, None), P(ALL, None), P(), P(), P(), P(), P(None, None, TP), P(), P(), P(None, TP, None)),
        out_specs=P(ALL, None),
        check_vma=False,
    )
```

```python
import functools

import jax
import jax.numpy as jnp
from jax import lax
from jax.experimental import pallas as pl
from jax.experimental.pallas import tpu as pltpu
from jax.sharding import Mesh
from jax.sharding import PartitionSpec as P

ROWS = ("z", "y")
TP = ("x", "c")
ALL = ("z", "y", "x", "c")
EPS = 1e-06
LOG2E = 1.4426950408889634
F32 = jnp.float32
BF16 = jnp.bfloat16


def dot(a, b):
    return jnp.dot(a, b, preferred_element_type=F32)


def dot_t(a, b):
    return lax.dot_general(a, b, (((1,), (1,)), ((), ())), preferred_element_type=F32)


def rms(value):
    return lax.rsqrt(jnp.mean(value * value, axis=-1, keepdims=True) + EPS)


def head_norm(value, gain_row, head):
    rows, width = value.shape
    low = lax.broadcasted_iota(jnp.int32, (rows, 2 * head), 1) < head
    groups = []
    for start in range(0, width, 2 * head):
        part = value[:, start : start + 2 * head]
        square = part * part
        first = jnp.sum(jnp.where(low, square, 0.0), axis=-1, keepdims=True)
        second = jnp.sum(jnp.where(low, 0.0, square), axis=-1, keepdims=True)
        scale = lax.rsqrt(jnp.where(low, first, second) / head + EPS)
        groups.append(part * scale * gain_row)
    return groups


def doubled(row):
    return jnp.concatenate([row, row], axis=-1)


def source_kernel(source, gain, key_gain, key_weight, value_weight, out):
    layers, head = key_gain.shape
    value = source[...].astype(F32)
    scaled = value * rms(value)
    width = key_weight.shape[2]
    for layer in range(layers):
        normed = (scaled * gain[layer : layer + 1, :]).astype(BF16)
        keys = dot(normed, key_weight[layer])
        row = doubled(key_gain[layer : layer + 1, :])
        groups = head_norm(keys, row, head)
        for k, group in enumerate(groups):
            out[layer, :, k * 2 * head : (k + 1) * 2 * head] = group.astype(BF16)
        out[layer, :, width:] = dot(normed, value_weight[layer]).astype(BF16)


def store_groups(out, groups):
    width = groups[0].shape[1]
    for k, group in enumerate(groups):
        out[:, k * width : (k + 1) * width] = group.astype(BF16)


def project(value, gain_row, weight, query_gain, layer, out):
    head = query_gain.shape[1]
    normed = (value * rms(value) * gain_row).astype(BF16)
    row = doubled(query_gain[layer : layer + 1, :])
    store_groups(out, head_norm(dot_t(normed, weight[...]), row, head))


def query_kernel(layer, target, gain, query_gain, weight, out):
    project(target[...].astype(F32), gain[layer : layer + 1, :], weight, query_gain, layer, out)


def mixed(arrived, hidden, weight, heads, head):
    total = arrived[0].astype(F32)
    for k in range(1, arrived.shape[0]):
        total = total + arrived[k].astype(F32)
    rows = total.shape[0]
    width = heads * head
    mass = total[:, width : width + heads] + total[:, width + heads : width + 2 * heads]
    low = lax.broadcasted_iota(jnp.int32, (rows, 2 * head), 1) < head
    branch = None
    for g in range(heads // 2):
        below = jnp.where(low, mass[:, 2 * g : 2 * g + 1], mass[:, 2 * g + 1 : 2 * g + 2])
        columns = slice(2 * g * head, 2 * (g + 1) * head)
        part = dot((total[:, columns] / below).astype(BF16), weight[columns, :])
        branch = part if branch is None else branch + part
    return (hidden[...].astype(F32) + branch).astype(BF16)


def middle_kernel(layer, heads, arrived, hidden, gain, query_gain, out_weight, weight, hidden_out, out):
    now = mixed(arrived, hidden, out_weight, heads, query_gain.shape[1])
    hidden_out[...] = now
    project(now.astype(F32), gain[layer : layer + 1, :], weight, query_gain, layer, out)


def last_kernel(heads, head, arrived, hidden, out_weight, hidden_out):
    hidden_out[...] = mixed(arrived, hidden, out_weight, heads, head)


def attention_kernel(heads, head, tile, queries, pairs, out, rhs, value_t, gathered):
    keys = pairs.shape[0]
    width = 2 * head
    columns = queries.shape[0]
    factor = LOG2E * head**-0.5
    turned = jnp.transpose(queries[...].astype(F32)).astype(BF16)
    zero = jnp.zeros((head, columns), BF16)
    per = heads // 2
    for p in range(heads):
        kv = p // per
        rhs[p, kv * head : (kv + 1) * head, :] = turned[p * head : (p + 1) * head, :]
        rhs[p, (1 - kv) * head : (2 - kv) * head, :] = zero
    value_t[...] = jnp.transpose(pairs[:, width:].astype(F32)).astype(BF16)
    for kv in range(2):

        def one_head(j, carry, kv=kv):
            p = kv * per + j
            right = rhs[p]
            mass = jnp.zeros((8, columns), F32)
            total = None
            for t in range(keys // tile):
                score = dot(pairs[t * tile : (t + 1) * tile, :width], right)
                weight = jnp.exp2(score * factor)
                mass = mass + jnp.sum(weight.reshape(tile // 8, 8, columns), axis=0)
                part = dot(value_t[:, t * tile : (t + 1) * tile], weight.astype(BF16))
                total = part if total is None else total + part
            gathered[pl.ds(pl.multiple_of(p * head, head), head), :] = total[kv * head : (kv + 1) * head, :]
            mass = jnp.sum(mass, axis=0, keepdims=True)
            top = mass.astype(BF16).astype(F32)
            gathered[pl.ds(heads * head + p, 1), :] = top
            gathered[pl.ds(heads * head + heads + p, 1), :] = mass - top
            return carry

        lax.fori_loop(0, per, one_head, 0)
    rest = heads * head + 2 * heads
    gathered[rest:, :] = jnp.zeros((gathered.shape[0] - rest, columns), F32)
    out[...] = jnp.transpose(gathered[...]).astype(BF16)


def call(kernel, shapes, scratch=(), flops=1000000):
    one = not isinstance(shapes, (list, tuple))
    specs = pl.BlockSpec(memory_space=pltpu.VMEM)
    return pl.pallas_call(
        kernel,
        out_shape=shapes,
        out_specs=specs if one else [specs] * len(shapes),
        scratch_shapes=list(scratch),
        compiler_params=pltpu.CompilerParams(vmem_limit_bytes=40 * 1024 * 1024),
        cost_estimate=pl.CostEstimate(flops=flops, bytes_accessed=1000000, transcendentals=0),
    )


def to_all(value, axis):
    copies = jnp.broadcast_to(value, (lax.axis_size(axis), *value.shape))
    return lax.all_to_all(copies, axis, split_axis=0, concat_axis=0, tiled=True)


def body(target, source, target_gain, source_gain, query_gain, key_gain, query_weight, key_weight, value_weight, out_weight):
    layers, _, head_columns = query_weight.shape
    head = query_gain.shape[1]
    heads = head_columns // head * lax.axis_size(TP)
    rows, model = target.shape
    group = rows * lax.axis_size(TP)
    shapes = jax.ShapeDtypeStruct
    query_t = jnp.swapaxes(query_weight, 1, 2)
    width = heads * head
    wide = width + 128

    with jax.named_scope("keys"):
        pairs = call(source_kernel, shapes((layers, rows, 4 * head), BF16), flops=200000000)(
            source, source_gain, key_gain, key_weight, value_weight
        )
        plane = to_all(pairs, "z")
        columns = [plane[:, layer].reshape(-1, 4 * head) for layer in range(layers)]

    def full(piece, name):
        with jax.named_scope(name):
            return lax.all_gather(piece, TP, tiled=True)

    def line(piece, name):
        with jax.named_scope(name):
            return lax.all_gather(piece, "y", tiled=True)

    query_full = [full(query_t[0], "wq0")]
    arrived_pairs = [line(columns[0], "kv0")]
    out_full = [full(out_weight[0], "wo0")]
    query_full.append(full(query_t[1], "wq1"))
    arrived_pairs.append(line(columns[1], "kv1"))
    out_full.append(full(out_weight[1], "wo1"))

    queries = call(functools.partial(query_kernel, 0), shapes((rows, width), BF16), flops=200000000)(
        target, target_gain, query_gain, query_full[0]
    )
    hidden = target
    for layer in range(layers):
        everyone = to_all(queries, TP).reshape(group, width)
        kv = arrived_pairs[layer]
        partial = call(
            functools.partial(attention_kernel, heads, head, 256),
            shapes((group, wide), BF16),
            scratch=[
                pltpu.VMEM((heads, 2 * head, group), BF16),
                pltpu.VMEM((2 * head, kv.shape[0]), BF16),
                pltpu.VMEM((wide, group), F32),
            ],
            flops=5000000000,
        )(everyone, kv)
        arrived = lax.all_to_all(partial.reshape(-1, rows, wide), TP, split_axis=0, concat_axis=0, tiled=True)
        if layer + 1 < layers:
            hidden, queries = call(
                functools.partial(middle_kernel, layer + 1, heads),
                [shapes((rows, model), BF16), shapes((rows, width), BF16)],
                flops=400000000,
            )(arrived, hidden, target_gain, query_gain, out_full[layer], query_full[layer + 1])
        else:
            hidden = call(functools.partial(last_kernel, heads, head), shapes((rows, model), BF16), flops=200000000)(
                arrived, hidden, out_full[layer]
            )
    return hidden


def solution(mesh):
    columns = mesh.shape["tp"]
    split = Mesh(mesh.devices.reshape(8, 8, columns // 2, 2), ALL)
    return jax.shard_map(
        body,
        mesh=split,
        in_specs=(P(ALL, None), P(ALL, None), P(), P(), P(), P(), P(None, None, TP), P(), P(), P(None, TP, None)),
        out_specs=P(ALL, None),
        check_vma=False,
    )
```

```python
import functools

import jax
import jax.numpy as jnp
from jax import lax
from jax.experimental import pallas as pl
from jax.experimental.pallas import tpu as pltpu
from jax.sharding import Mesh
from jax.sharding import PartitionSpec as P

ROWS = ("z", "y")
TP = ("x", "c")
ALL = ("z", "y", "x", "c")
EPS = 1e-06
LOG2E = 1.4426950408889634
F32 = jnp.float32
BF16 = jnp.bfloat16


def dot(a, b):
    return jnp.dot(a, b, preferred_element_type=F32)


def dot_t(a, b):
    return lax.dot_general(a, b, (((1,), (1,)), ((), ())), preferred_element_type=F32)


def rms(value):
    return lax.rsqrt(jnp.mean(value * value, axis=-1, keepdims=True) + EPS)


def head_norm(value, gain_row, head):
    rows, width = value.shape
    low = lax.broadcasted_iota(jnp.int32, (rows, 2 * head), 1) < head
    groups = []
    for start in range(0, width, 2 * head):
        part = value[:, start : start + 2 * head]
        square = part * part
        first = jnp.sum(jnp.where(low, square, 0.0), axis=-1, keepdims=True)
        second = jnp.sum(jnp.where(low, 0.0, square), axis=-1, keepdims=True)
        scale = lax.rsqrt(jnp.where(low, first, second) / head + EPS)
        groups.append(part * scale * gain_row)
    return groups


def doubled(row):
    return jnp.concatenate([row, row], axis=-1)


def source_kernel(source, gain, key_gain, key_weight, value_weight, out):
    layers, head = key_gain.shape
    value = source[...].astype(F32)
    scaled = value * rms(value)
    width = key_weight.shape[2]
    for layer in range(layers):
        normed = (scaled * gain[layer : layer + 1, :]).astype(BF16)
        keys = dot(normed, key_weight[layer])
        row = doubled(key_gain[layer : layer + 1, :])
        groups = head_norm(keys, row, head)
        for k, group in enumerate(groups):
            out[layer, :, k * 2 * head : (k + 1) * 2 * head] = group.astype(BF16)
        out[layer, :, width:] = dot(normed, value_weight[layer]).astype(BF16)


def project(normed, mine, other, row, head, place):
    x, core = place[0], place[1]
    model = normed.shape[1]
    own = jnp.concatenate(head_norm(dot_t(normed, mine.reshape(-1, model)), row, head), axis=1)
    far = jnp.concatenate(head_norm(dot_t(normed, other.reshape(-1, model)), row, head), axis=1)
    own = pltpu.roll(own, x * head, 1)
    far = pltpu.roll(far, x * head, 1)
    return jnp.where(core == 0, own, far), jnp.where(core == 0, far, own)


def store_groups(out, groups):
    width = groups[0].shape[1]
    for k, group in enumerate(groups):
        out[:, k * width : (k + 1) * width] = group.astype(BF16)


def query_kernel(layer, place, target, gain, query_gain, mine, other, out):
    head = query_gain.shape[1]
    value = target[...].astype(F32)
    normed = (value * rms(value) * gain[layer : layer + 1, :]).astype(BF16)
    row = doubled(query_gain[layer : layer + 1, :])
    store_groups(out, project(normed, mine[...], other[...], row, head, place))


def attended_halves(arrived, heads, head):
    total = arrived[0].astype(F32)
    for k in range(1, arrived.shape[0]):
        total = total + arrived[k].astype(F32)
    rows = total.shape[0]
    width = heads * head
    mass = total[:, width : width + heads] + total[:, width + heads : width + 2 * heads]
    low = lax.broadcasted_iota(jnp.int32, (rows, 2 * head), 1) < head
    groups = []
    for g in range(heads // 2):
        below = jnp.where(low, mass[:, 2 * g : 2 * g + 1], mass[:, 2 * g + 1 : 2 * g + 2])
        groups.append(total[:, 2 * g * head : 2 * (g + 1) * head] / below)
    half = len(groups) // 2
    return jnp.concatenate(groups[:half], axis=1), jnp.concatenate(groups[half:], axis=1)


def mixed(place, arrived, hidden, mine, other, heads, head):
    x, core = place[0], place[1]
    even, odd = attended_halves(arrived, heads, head)
    width = even.shape[1]
    back = (width - x * head) % width
    own = pltpu.roll(jnp.where(core == 0, even, odd), back, 1).astype(BF16)
    far = pltpu.roll(jnp.where(core == 0, odd, even), back, 1).astype(BF16)
    model = hidden.shape[1]
    branch = dot(own, mine[...].reshape(-1, model)) + dot(far, other[...].reshape(-1, model))
    return (hidden[...].astype(F32) + branch).astype(BF16)


def middle_kernel(layer, heads, place, arrived, hidden, gain, query_gain, out_mine, out_other, mine, other, hidden_out, out):
    head = query_gain.shape[1]
    now = mixed(place, arrived, hidden, out_mine, out_other, heads, head)
    hidden_out[...] = now
    value = now.astype(F32)
    normed = (value * rms(value) * gain[layer : layer + 1, :]).astype(BF16)
    row = doubled(query_gain[layer : layer + 1, :])
    store_groups(out, project(normed, mine[...], other[...], row, head, place))


def last_kernel(heads, head, place, arrived, hidden, out_mine, out_other, hidden_out):
    hidden_out[...] = mixed(place, arrived, hidden, out_mine, out_other, heads, head)


def attention_kernel(heads, head, tile, count, place, *refs):
    queries, (pairs, out, rhs, value_t, gathered) = refs[:count], refs[count:]
    blocks, each_rows, _ = pairs.shape
    keys = blocks * each_rows
    width = 2 * head
    everyone = jnp.concatenate([part[...].astype(F32) for part in queries], axis=0)
    columns = everyone.shape[0]
    factor = LOG2E * head**-0.5
    turned = jnp.transpose(everyone).astype(BF16)
    zero = jnp.zeros((head, columns), BF16)
    per = heads // 4
    for p in range(heads):
        kv = (p % 4) // 2
        rhs[p, kv * head : (kv + 1) * head, :] = turned[p * head : (p + 1) * head, :]
        rhs[p, (1 - kv) * head : (2 - kv) * head, :] = zero
    value_t[...] = jnp.transpose(pairs[:, :, width:].reshape(keys, width).astype(F32)).astype(BF16)
    for kv in range(2):

        def one_head(j, carry, kv=kv):
            p = (j // 2) * 4 + 2 * kv + j % 2
            right = rhs[p]
            mass = jnp.zeros((8, columns), F32)
            total = None
            for t in range(keys // tile):
                taken = slice(t * tile // each_rows, (t + 1) * tile // each_rows)
                score = dot(pairs[taken, :, :width].reshape(tile, width), right)
                weight = jnp.exp2(score * factor)
                mass = mass + jnp.sum(weight.reshape(tile // 8, 8, columns), axis=0)
                part = dot(value_t[:, t * tile : (t + 1) * tile], weight.astype(BF16))
                total = part if total is None else total + part
            gathered[pl.ds(pl.multiple_of(p * head, head), head), :] = total[kv * head : (kv + 1) * head, :]
            mass = jnp.sum(mass, axis=0, keepdims=True)
            top = mass.astype(BF16).astype(F32)
            gathered[pl.ds(heads * head + p, 1), :] = top
            gathered[pl.ds(heads * head + heads + p, 1), :] = mass - top
            return carry

        lax.fori_loop(0, 2 * per, one_head, 0)
    rest = heads * head + 2 * heads
    gathered[rest:, :] = jnp.zeros((gathered.shape[0] - rest, columns), F32)
    result = jnp.transpose(gathered[...]).astype(BF16)
    if count == 1:
        out[...] = result
        return
    each = columns // (2 * count)
    for r in range(count):
        for d in range(2):
            to = ((place[0] + r) % count) * 2 + (place[1] + d) % 2
            first = (2 * r + d) * each
            out[pl.ds(pl.multiple_of(to * each, each), each), :] = result[first : first + each, :]


def call(kernel, shapes, scratch=(), flops=1000000):
    one = not isinstance(shapes, (list, tuple))
    specs = pl.BlockSpec(memory_space=pltpu.VMEM)
    return pl.pallas_call(
        kernel,
        out_shape=shapes,
        out_specs=specs if one else [specs] * len(shapes),
        scratch_shapes=list(scratch),
        compiler_params=pltpu.CompilerParams(vmem_limit_bytes=40 * 1024 * 1024),
        cost_estimate=pl.CostEstimate(flops=flops, bytes_accessed=1000000, transcendentals=0),
    )


def whole(value):
    return pl.BlockSpec(value.shape, lambda i, n=value.ndim: (0,) * n)


def part_of(value, k, size):
    if value.ndim == 4:
        return pl.BlockSpec((value.shape[0], None, *value.shape[2:]), lambda i, k=k: (0, k, 0, 0))
    return pl.BlockSpec((value.shape[0], size, value.shape[2]), lambda i, k=k: (0, k, 0))


def with_place(kernel, shapes, operands, parts, flops, scratch=()):
    one = not isinstance(shapes, (list, tuple))
    place, *rest = operands
    specs = [pl.BlockSpec(memory_space=pltpu.SMEM)] + [whole(value) for value in rest]
    specs += [part_of(*part) for part in parts]
    return pl.pallas_call(
        kernel,
        grid=(1,),
        out_shape=shapes,
        in_specs=specs,
        out_specs=whole(shapes) if one else [whole(shape) for shape in shapes],
        scratch_shapes=list(scratch),
        compiler_params=pltpu.CompilerParams(vmem_limit_bytes=40 * 1024 * 1024),
        cost_estimate=pl.CostEstimate(flops=flops, bytes_accessed=1000000, transcendentals=0),
    )(place, *rest, *(part[0] for part in parts))


def to_all(value, axis):
    copies = jnp.broadcast_to(value, (lax.axis_size(axis), *value.shape))
    return lax.all_to_all(copies, axis, split_axis=0, concat_axis=0, tiled=True)


def shifted(value, axis, step):
    size = lax.axis_size(axis)
    return lax.ppermute(value, axis, [((k + step) % size, k) for k in range(size)])


def around(value):
    half = value.shape[0] // 2
    right, left = shifted(value, "x", 1), shifted(value, "x", -1)
    far = [shifted(right[:half], "x", 1), shifted(left[half:], "x", -1)]
    return jnp.concatenate([value, right, *far, left], axis=0).reshape(4, *value.shape)


def decoder(target, source, target_gain, source_gain, query_gain, key_gain, query_weight, key_weight, value_weight, out_weight):
    layers, _, head_columns = query_weight.shape
    head = query_gain.shape[1]
    heads = head_columns // head * lax.axis_size(TP)
    rows, model = target.shape
    group = rows * lax.axis_size(TP)
    shapes = jax.ShapeDtypeStruct
    place = jnp.stack([lax.axis_index("x"), lax.axis_index("c")])
    query_t = jnp.swapaxes(query_weight, 1, 2)
    width = heads * head
    wide = width + 128

    pairs = call(source_kernel, shapes((layers, rows, 4 * head), BF16), flops=200000000)(
        source, source_gain, key_gain, key_weight, value_weight
    )
    plane = to_all(pairs, ROWS)
    keys = plane.shape[0] * rows

    def both(stacked):
        return stacked, shifted(stacked, "c", 1)

    first = both(around(query_t[0]))
    rest = both(around(jnp.concatenate([out_weight[0], query_t[1], out_weight[1]], axis=0)))
    rest = [[(part, k, head) for part in rest] for k in range(3)]

    queries = with_place(
        functools.partial(query_kernel, 0),
        shapes((rows, width), BF16),
        (place, target, target_gain, query_gain),
        [(part, 0, head) for part in first],
        200000000,
    )
    chip = jnp.concatenate([queries, shifted(queries, "c", 1)], axis=0)
    everyone = [chip] + [shifted(chip, "x", k) for k in range(1, lax.axis_size("x"))]

    hidden = target
    for layer in range(layers):
        partial = with_place(
            functools.partial(attention_kernel, heads, head, 256, len(everyone)),
            shapes((group, wide), BF16),
            (place, *everyone),
            [(plane, layer, 1)],
            5000000000,
            scratch=[
                pltpu.VMEM((heads, 2 * head, group), BF16),
                pltpu.VMEM((2 * head, keys), BF16),
                pltpu.VMEM((wide, group), F32),
            ],
        )
        arrived = lax.all_to_all(partial.reshape(-1, rows, wide), TP, split_axis=0, concat_axis=0, tiled=True)
        if layer + 1 < layers:
            hidden, queries = with_place(
                functools.partial(middle_kernel, layer + 1, heads),
                [shapes((rows, model), BF16), shapes((rows, width), BF16)],
                (place, arrived, hidden, target_gain, query_gain),
                rest[0] + rest[1],
                400000000,
            )
            everyone = [to_all(queries, TP).reshape(group, width)]
        else:
            hidden = with_place(
                functools.partial(last_kernel, heads, head),
                shapes((rows, model), BF16),
                (place, arrived, hidden),
                rest[2],
                200000000,
            )
    return hidden


def solution(mesh):
    columns = mesh.shape["tp"]
    split = Mesh(mesh.devices.reshape(8, 8, columns // 2, 2), ALL)
    return jax.shard_map(
        decoder,
        mesh=split,
        in_specs=(P(ALL, None), P(ALL, None), P(), P(), P(), P(), P(None, None, TP), P(), P(), P(None, TP, None)),
        out_specs=P(ALL, None),
        check_vma=False,
    )
```

```python
import functools

import jax
import jax.numpy as jnp
from jax import lax
from jax.experimental import pallas as pl
from jax.experimental.pallas import tpu as pltpu
from jax.sharding import Mesh
from jax.sharding import PartitionSpec as P

ROWS = ("z", "y")
TP = ("x", "c")
ALL = ("z", "y", "x", "c")
EPS = 1e-06
LOG2E = 1.4426950408889634
F32 = jnp.float32
BF16 = jnp.bfloat16


def dot(a, b):
    return jnp.dot(a, b, preferred_element_type=F32)


def dot_t(a, b):
    return lax.dot_general(a, b, (((1,), (1,)), ((), ())), preferred_element_type=F32)


def rms(value):
    return lax.rsqrt(jnp.mean(value * value, axis=-1, keepdims=True) + EPS)


def head_norm(value, gain_row, head):
    rows, width = value.shape
    low = lax.broadcasted_iota(jnp.int32, (rows, 2 * head), 1) < head
    groups = []
    for start in range(0, width, 2 * head):
        part = value[:, start : start + 2 * head]
        square = part * part
        first = jnp.sum(jnp.where(low, square, 0.0), axis=-1, keepdims=True)
        second = jnp.sum(jnp.where(low, 0.0, square), axis=-1, keepdims=True)
        scale = lax.rsqrt(jnp.where(low, first, second) / head + EPS)
        groups.append(part * scale * gain_row)
    return groups


def doubled(row):
    return jnp.concatenate([row, row], axis=-1)


def source_kernel(source, gain, key_gain, key_weight, value_weight, out):
    layers, head = key_gain.shape
    value = source[...].astype(F32)
    scaled = value * rms(value)
    width = key_weight.shape[2]
    for layer in range(layers):
        normed = (scaled * gain[layer : layer + 1, :]).astype(BF16)
        keys = dot(normed, key_weight[layer])
        row = doubled(key_gain[layer : layer + 1, :])
        groups = head_norm(keys, row, head)
        for k, group in enumerate(groups):
            out[layer, :, k * 2 * head : (k + 1) * 2 * head] = group.astype(BF16)
        out[layer, :, width:] = dot(normed, value_weight[layer]).astype(BF16)


def project(normed, mine, other, row, head, place, turned=True):
    x, core = place[0], place[1]
    model = normed.shape[1]
    own = jnp.concatenate(head_norm(dot_t(normed, mine.reshape(-1, model)), row, head), axis=1)
    far = jnp.concatenate(head_norm(dot_t(normed, other.reshape(-1, model)), row, head), axis=1)
    if turned:
        own = pltpu.roll(own, x * head, 1)
        far = pltpu.roll(far, x * head, 1)
    return jnp.where(core == 0, own, far), jnp.where(core == 0, far, own)


def store_groups(out, groups):
    width = groups[0].shape[1]
    for k, group in enumerate(groups):
        out[:, k * width : (k + 1) * width] = group.astype(BF16)


def query_kernel(layer, place, target, gain, query_gain, mine, other, out):
    head = query_gain.shape[1]
    value = target[...].astype(F32)
    normed = (value * rms(value) * gain[layer : layer + 1, :]).astype(BF16)
    row = doubled(query_gain[layer : layer + 1, :])
    store_groups(out, project(normed, mine[...], other[...], row, head, place, turned=False))


def attended_halves(arrived, heads, head):
    total = arrived[0].astype(F32)
    for k in range(1, arrived.shape[0]):
        total = total + arrived[k].astype(F32)
    rows = total.shape[0]
    width = heads * head
    mass = total[:, width : width + heads] + total[:, width + heads : width + 2 * heads]
    low = lax.broadcasted_iota(jnp.int32, (rows, 2 * head), 1) < head
    groups = []
    for g in range(heads // 2):
        below = jnp.where(low, mass[:, 2 * g : 2 * g + 1], mass[:, 2 * g + 1 : 2 * g + 2])
        groups.append(total[:, 2 * g * head : 2 * (g + 1) * head] / below)
    half = len(groups) // 2
    return jnp.concatenate(groups[:half], axis=1), jnp.concatenate(groups[half:], axis=1)


def mixed(place, arrived, hidden, mine, other, heads, head):
    x, core = place[0], place[1]
    even, odd = attended_halves(arrived, heads, head)
    width = even.shape[1]
    back = (width - x * head) % width
    own = pltpu.roll(jnp.where(core == 0, even, odd), back, 1).astype(BF16)
    far = pltpu.roll(jnp.where(core == 0, odd, even), back, 1).astype(BF16)
    model = hidden.shape[1]
    branch = dot(own, mine[...].reshape(-1, model)) + dot(far, other[...].reshape(-1, model))
    return (hidden[...].astype(F32) + branch).astype(BF16)


def middle_kernel(layer, heads, place, arrived, hidden, gain, query_gain, out_mine, out_other, mine, other, hidden_out, out):
    head = query_gain.shape[1]
    now = mixed(place, arrived, hidden, out_mine, out_other, heads, head)
    hidden_out[...] = now
    value = now.astype(F32)
    normed = (value * rms(value) * gain[layer : layer + 1, :]).astype(BF16)
    row = doubled(query_gain[layer : layer + 1, :])
    store_groups(out, project(normed, mine[...], other[...], row, head, place))


def last_kernel(heads, head, place, arrived, hidden, out_mine, out_other, hidden_out):
    hidden_out[...] = mixed(place, arrived, hidden, out_mine, out_other, heads, head)


def attention_kernel(heads, head, tile, count, place, *refs):
    queries, (pairs, out, rhs, value_t, gathered) = refs[:count], refs[count:]
    blocks, each_rows, _ = pairs.shape
    keys = blocks * each_rows
    width = 2 * head
    everyone = jnp.concatenate([part[...].astype(F32) for part in queries], axis=0)
    columns = everyone.shape[0]
    factor = LOG2E * head**-0.5
    turned = jnp.transpose(everyone).astype(BF16)
    zero = jnp.zeros((head, columns), BF16)
    per = heads // 4
    for p in range(heads):
        kv = (p % 4) // 2
        rhs[p, kv * head : (kv + 1) * head, :] = turned[p * head : (p + 1) * head, :]
        rhs[p, (1 - kv) * head : (2 - kv) * head, :] = zero
    value_t[...] = jnp.transpose(pairs[:, :, width:].reshape(keys, width).astype(F32)).astype(BF16)
    for kv in range(2):

        def one_head(j, carry, kv=kv):
            p = (j // 2) * 4 + 2 * kv + j % 2
            right = rhs[p]
            mass = jnp.zeros((8, columns), F32)
            total = None
            for t in range(keys // tile):
                taken = slice(t * tile // each_rows, (t + 1) * tile // each_rows)
                score = dot(pairs[taken, :, :width].reshape(tile, width), right)
                weight = jnp.exp2(score * factor)
                mass = mass + jnp.sum(weight.reshape(tile // 8, 8, columns), axis=0)
                part = dot(value_t[:, t * tile : (t + 1) * tile], weight.astype(BF16))
                total = part if total is None else total + part
            gathered[pl.ds(pl.multiple_of(p * head, head), head), :] = total[kv * head : (kv + 1) * head, :]
            mass = jnp.sum(mass, axis=0, keepdims=True)
            top = mass.astype(BF16).astype(F32)
            gathered[pl.ds(heads * head + p, 1), :] = top
            gathered[pl.ds(heads * head + heads + p, 1), :] = mass - top
            return carry

        lax.fori_loop(0, 2 * per, one_head, 0)
    rest = heads * head + 2 * heads
    gathered[rest:, :] = jnp.zeros((gathered.shape[0] - rest, columns), F32)
    result = jnp.transpose(gathered[...]).astype(BF16)
    if count == 1:
        out[...] = result
        return
    each = columns // (2 * count)
    for r in range(count):
        for d in range(2):
            to = ((place[0] + r) % count) * 2 + (place[1] + d) % 2
            first = (2 * r + d) * each
            out[pl.ds(pl.multiple_of(to * each, each), each), :] = result[first : first + each, :]


def whole(value):
    return pl.BlockSpec(value.shape, lambda i, n=value.ndim: (0,) * n)


def part_of(value, k, size):
    if value.ndim == 4:
        return pl.BlockSpec((value.shape[0], None, *value.shape[2:]), lambda i, k=k: (0, k, 0, 0))
    return pl.BlockSpec((value.shape[0], size, value.shape[2]), lambda i, k=k: (0, k, 0))


def with_place(kernel, shapes, operands, parts, flops, scratch=()):
    one = not isinstance(shapes, (list, tuple))
    place, *rest = operands
    placed = [] if place is None else [place]
    specs = [pl.BlockSpec(memory_space=pltpu.SMEM)] * len(placed) + [whole(value) for value in rest]
    specs += [part_of(*part) for part in parts]
    return pl.pallas_call(
        kernel,
        grid=(1,),
        out_shape=shapes,
        in_specs=specs,
        out_specs=whole(shapes) if one else [whole(shape) for shape in shapes],
        scratch_shapes=list(scratch),
        compiler_params=pltpu.CompilerParams(vmem_limit_bytes=40 * 1024 * 1024),
        cost_estimate=pl.CostEstimate(flops=flops, bytes_accessed=1000000, transcendentals=0),
    )(*placed, *rest, *(part[0] for part in parts))


def to_all(value, axis):
    copies = jnp.broadcast_to(value, (lax.axis_size(axis), *value.shape))
    return lax.all_to_all(copies, axis, split_axis=0, concat_axis=0, tiled=True)


def shifted(value, axis, step):
    size = lax.axis_size(axis)
    return lax.ppermute(value, axis, [((k + step) % size, k) for k in range(size)])


def around(value):
    half = value.shape[0] // 2
    right, left = shifted(value, "x", 1), shifted(value, "x", -1)
    far = [shifted(right[:half], "x", 1), shifted(left[half:], "x", -1)]
    return jnp.concatenate([value, right, *far, left], axis=0).reshape(4, *value.shape)


def decoder(target, source, target_gain, source_gain, query_gain, key_gain, query_weight, key_weight, value_weight, out_weight):
    layers, _, head_columns = query_weight.shape
    head = query_gain.shape[1]
    heads = head_columns // head * lax.axis_size(TP)
    rows, model = target.shape
    group = rows * lax.axis_size(TP)
    shapes = jax.ShapeDtypeStruct
    place = jnp.stack([lax.axis_index("x"), lax.axis_index("c")])
    query_t = jnp.swapaxes(query_weight, 1, 2)
    width = heads * head
    wide = width + 128

    pairs = with_place(
        source_kernel,
        shapes((layers, rows, 4 * head), BF16),
        (None, source, source_gain, key_gain, key_weight, value_weight),
        [],
        200000000,
    )
    plane = to_all(pairs, ROWS)
    keys = plane.shape[0] * rows

    def both(stacked):
        return stacked, shifted(stacked, "c", 1)

    first = both(to_all(query_t[0], "x"))
    rest = both(around(jnp.concatenate([out_weight[0], query_t[1], out_weight[1]], axis=0)))
    rest = [[(part, k, head) for part in rest] for k in range(3)]

    queries = with_place(
        functools.partial(query_kernel, 0),
        shapes((rows, width), BF16),
        (place, target, target_gain, query_gain),
        [(part, 0, head) for part in first],
        200000000,
    )
    chip = jnp.concatenate([queries, shifted(queries, "c", 1)], axis=0)
    everyone = [chip] + [shifted(chip, "x", k) for k in range(1, lax.axis_size("x"))]

    hidden = target
    for layer in range(layers):
        partial = with_place(
            functools.partial(attention_kernel, heads, head, 256, len(everyone)),
            shapes((group, wide), BF16),
            (place, *everyone),
            [(plane, layer, 1)],
            5000000000,
            scratch=[
                pltpu.VMEM((heads, 2 * head, group), BF16),
                pltpu.VMEM((2 * head, keys), BF16),
                pltpu.VMEM((wide, group), F32),
            ],
        )
        arrived = lax.all_to_all(partial.reshape(-1, rows, wide), TP, split_axis=0, concat_axis=0, tiled=True)
        if layer + 1 < layers:
            hidden, queries = with_place(
                functools.partial(middle_kernel, layer + 1, heads),
                [shapes((rows, model), BF16), shapes((rows, width), BF16)],
                (place, arrived, hidden, target_gain, query_gain),
                rest[0] + rest[1],
                400000000,
            )
            everyone = [to_all(queries, TP).reshape(group, width)]
        else:
            hidden = with_place(
                functools.partial(last_kernel, heads, head),
                shapes((rows, model), BF16),
                (place, arrived, hidden),
                rest[2],
                200000000,
            )
    return hidden


def solution(mesh):
    columns = mesh.shape["tp"]
    split = Mesh(mesh.devices.reshape(8, 8, columns // 2, 2), ALL)
    return jax.shard_map(
        decoder,
        mesh=split,
        in_specs=(P(ALL, None), P(ALL, None), P(), P(), P(), P(), P(None, None, TP), P(), P(), P(None, TP, None)),
        out_specs=P(ALL, None),
        check_vma=False,
    )
```

```python
import functools

import jax
import jax.numpy as jnp
from jax import lax
from jax.experimental import pallas as pl
from jax.experimental.pallas import tpu as pltpu
from jax.sharding import Mesh
from jax.sharding import PartitionSpec as P

ROWS = ("z", "y")
TP = ("x", "c")
ALL = ("z", "y", "x", "c")
EPS = 1e-06
LOG2E = 1.4426950408889634
F32 = jnp.float32
BF16 = jnp.bfloat16


def dot(a, b):
    return jnp.dot(a, b, preferred_element_type=F32)


def dot_t(a, b):
    return lax.dot_general(a, b, (((1,), (1,)), ((), ())), preferred_element_type=F32)


def rms(value):
    return lax.rsqrt(jnp.mean(value * value, axis=-1, keepdims=True) + EPS)


def head_norm(value, gain_row, head):
    rows, width = value.shape
    low = lax.broadcasted_iota(jnp.int32, (rows, 2 * head), 1) < head
    groups = []
    for start in range(0, width, 2 * head):
        part = value[:, start : start + 2 * head]
        square = part * part
        first = jnp.sum(jnp.where(low, square, 0.0), axis=-1, keepdims=True)
        second = jnp.sum(jnp.where(low, 0.0, square), axis=-1, keepdims=True)
        scale = lax.rsqrt(jnp.where(low, first, second) / head + EPS)
        groups.append(part * scale * gain_row)
    return groups


def doubled(row):
    return jnp.concatenate([row, row], axis=-1)


def source_kernel(source, gain, key_gain, key_weight, value_weight, out):
    layers, head = key_gain.shape
    value = source[...].astype(F32)
    scaled = value * rms(value)
    width = key_weight.shape[2]
    for layer in range(layers):
        normed = (scaled * gain[layer : layer + 1, :]).astype(BF16)
        keys = dot(normed, key_weight[layer])
        row = doubled(key_gain[layer : layer + 1, :])
        groups = head_norm(keys, row, head)
        for k, group in enumerate(groups):
            out[layer, :, k * 2 * head : (k + 1) * 2 * head] = group.astype(BF16)
        out[layer, :, width:] = dot(normed, value_weight[layer]).astype(BF16)


def project(normed, mine, other, row, head, place):
    x, core = place[0], place[1]
    model = normed.shape[1]
    own = jnp.concatenate(head_norm(dot_t(normed, mine.reshape(-1, model)), row, head), axis=1)
    far = jnp.concatenate(head_norm(dot_t(normed, other.reshape(-1, model)), row, head), axis=1)
    own = pltpu.roll(own, x * head, 1)
    far = pltpu.roll(far, x * head, 1)
    return jnp.where(core == 0, own, far), jnp.where(core == 0, far, own)


def store_groups(out, groups):
    width = groups[0].shape[1]
    for k, group in enumerate(groups):
        out[:, k * width : (k + 1) * width] = group.astype(BF16)


def query_kernel(layer, place, target, gain, query_gain, mine, other, out):
    head = query_gain.shape[1]
    value = target[...].astype(F32)
    normed = (value * rms(value) * gain[layer : layer + 1, :]).astype(BF16)
    row = doubled(query_gain[layer : layer + 1, :])
    store_groups(out, project(normed, mine[...], other[...], row, head, place))


def attended_halves(arrived, heads, head):
    total = arrived[0].astype(F32)
    for k in range(1, arrived.shape[0]):
        total = total + arrived[k].astype(F32)
    rows = total.shape[0]
    width = heads * head
    mass = total[:, width : width + heads] + total[:, width + heads : width + 2 * heads]
    low = lax.broadcasted_iota(jnp.int32, (rows, 2 * head), 1) < head
    groups = []
    for g in range(heads // 2):
        below = jnp.where(low, mass[:, 2 * g : 2 * g + 1], mass[:, 2 * g + 1 : 2 * g + 2])
        groups.append(total[:, 2 * g * head : 2 * (g + 1) * head] / below)
    half = len(groups) // 2
    return jnp.concatenate(groups[:half], axis=1), jnp.concatenate(groups[half:], axis=1)


def mixed(place, arrived, hidden, mine, other, heads, head):
    x, core = place[0], place[1]
    even, odd = attended_halves(arrived, heads, head)
    width = even.shape[1]
    back = (width - x * head) % width
    own = pltpu.roll(jnp.where(core == 0, even, odd), back, 1).astype(BF16)
    far = pltpu.roll(jnp.where(core == 0, odd, even), back, 1).astype(BF16)
    model = hidden.shape[1]
    branch = dot(own, mine[...].reshape(-1, model)) + dot(far, other[...].reshape(-1, model))
    return (hidden[...].astype(F32) + branch).astype(BF16)


def middle_kernel(layer, heads, place, arrived, hidden, gain, query_gain, out_mine, out_other, mine, other, hidden_out, out):
    head = query_gain.shape[1]
    now = mixed(place, arrived, hidden, out_mine, out_other, heads, head)
    hidden_out[...] = now
    value = now.astype(F32)
    normed = (value * rms(value) * gain[layer : layer + 1, :]).astype(BF16)
    row = doubled(query_gain[layer : layer + 1, :])
    store_groups(out, project(normed, mine[...], other[...], row, head, place))


def last_kernel(heads, head, place, arrived, hidden, out_mine, out_other, hidden_out):
    hidden_out[...] = mixed(place, arrived, hidden, out_mine, out_other, heads, head)


def attention_kernel(heads, head, tile, count, place, *refs):
    queries, (pairs, out, rhs, value_t, gathered) = refs[:count], refs[count:]
    blocks, each_rows, _ = pairs.shape
    keys = blocks * each_rows
    width = 2 * head
    everyone = jnp.concatenate([part[...].astype(F32) for part in queries], axis=0)
    columns = everyone.shape[0]
    factor = LOG2E * head**-0.5
    turned = jnp.transpose(everyone).astype(BF16)
    zero = jnp.zeros((head, columns), BF16)
    per = heads // 4
    for p in range(heads):
        kv = (p % 4) // 2
        rhs[p, kv * head : (kv + 1) * head, :] = turned[p * head : (p + 1) * head, :]
        rhs[p, (1 - kv) * head : (2 - kv) * head, :] = zero
    value_t[...] = jnp.transpose(pairs[:, :, width:].reshape(keys, width).astype(F32)).astype(BF16)
    for kv in range(2):

        def one_head(j, carry, kv=kv):
            p = (j // 2) * 4 + 2 * kv + j % 2
            right = rhs[p]
            mass = jnp.zeros((8, columns), F32)
            total = None
            for t in range(keys // tile):
                taken = slice(t * tile // each_rows, (t + 1) * tile // each_rows)
                score = dot(pairs[taken, :, :width].reshape(tile, width), right)
                weight = jnp.exp2(score * factor)
                mass = mass + jnp.sum(weight.reshape(tile // 8, 8, columns), axis=0)
                part = dot(value_t[:, t * tile : (t + 1) * tile], weight.astype(BF16))
                total = part if total is None else total + part
            gathered[pl.ds(pl.multiple_of(p * head, head), head), :] = total[kv * head : (kv + 1) * head, :]
            mass = jnp.sum(mass, axis=0, keepdims=True)
            top = mass.astype(BF16).astype(F32)
            gathered[pl.ds(heads * head + p, 1), :] = top
            gathered[pl.ds(heads * head + heads + p, 1), :] = mass - top
            return carry

        lax.fori_loop(0, 2 * per, one_head, 0)
    rest = heads * head + 2 * heads
    gathered[rest:, :] = jnp.zeros((gathered.shape[0] - rest, columns), F32)
    result = jnp.transpose(gathered[...]).astype(BF16)
    if count == 1:
        out[...] = result
        return
    each = columns // (2 * count)
    for r in range(count):
        for d in range(2):
            to = ((place[0] + r) % count) * 2 + (place[1] + d) % 2
            first = (2 * r + d) * each
            out[pl.ds(pl.multiple_of(to * each, each), each), :] = result[first : first + each, :]


def whole(value):
    return pl.BlockSpec(value.shape, lambda i, n=value.ndim: (0,) * n)


def part_of(value, k, size):
    if value.ndim == 4:
        return pl.BlockSpec((value.shape[0], None, *value.shape[2:]), lambda i, k=k: (0, k, 0, 0))
    return pl.BlockSpec((value.shape[0], size, value.shape[2]), lambda i, k=k: (0, k, 0))


def with_place(kernel, shapes, operands, parts, flops, scratch=(), limit=40):
    one = not isinstance(shapes, (list, tuple))
    place, *rest = operands
    placed = [] if place is None else [place]
    specs = [pl.BlockSpec(memory_space=pltpu.SMEM)] * len(placed) + [whole(value) for value in rest]
    specs += [part_of(*part) for part in parts]
    return pl.pallas_call(
        kernel,
        grid=(1,),
        out_shape=shapes,
        in_specs=specs,
        out_specs=whole(shapes) if one else [whole(shape) for shape in shapes],
        scratch_shapes=list(scratch),
        compiler_params=pltpu.CompilerParams(vmem_limit_bytes=limit * 1024 * 1024),
        cost_estimate=pl.CostEstimate(flops=flops, bytes_accessed=1000000, transcendentals=0),
    )(*placed, *rest, *(part[0] for part in parts))


def to_all(value, axis):
    copies = jnp.broadcast_to(value, (lax.axis_size(axis), *value.shape))
    return lax.all_to_all(copies, axis, split_axis=0, concat_axis=0, tiled=True)


def shifted(value, axis, step):
    size = lax.axis_size(axis)
    return lax.ppermute(value, axis, [((k + step) % size, k) for k in range(size)])


def around(value):
    half = value.shape[0] // 2
    right, left = shifted(value, "x", 1), shifted(value, "x", -1)
    far = [shifted(right[:half], "x", 1), shifted(left[half:], "x", -1)]
    return jnp.concatenate([value, right, *far, left], axis=0).reshape(4, *value.shape)


def decoder(target, source, target_gain, source_gain, query_gain, key_gain, query_weight, key_weight, value_weight, out_weight):
    layers, _, head_columns = query_weight.shape
    head = query_gain.shape[1]
    heads = head_columns // head * lax.axis_size(TP)
    rows, model = target.shape
    group = rows * lax.axis_size(TP)
    shapes = jax.ShapeDtypeStruct
    place = jnp.stack([lax.axis_index("x"), lax.axis_index("c")])
    query_t = jnp.swapaxes(query_weight, 1, 2)
    width = heads * head
    wide = width + 128

    pairs = with_place(
        source_kernel,
        shapes((layers, rows, 4 * head), BF16),
        (None, source, source_gain, key_gain, key_weight, value_weight),
        [],
        200000000,
        limit=63,
    )
    plane = to_all(pairs, ROWS)
    keys = plane.shape[0] * rows

    def both(stacked):
        return stacked, shifted(stacked, "c", 1)

    beside = [query_t[0]] + [shifted(query_t[0], "x", k) for k in range(1, lax.axis_size("x"))]
    first = both(jnp.stack(beside))
    rest = both(around(jnp.concatenate([out_weight[0], query_t[1], out_weight[1]], axis=0)))
    rest = [[(part, k, head) for part in rest] for k in range(3)]

    queries = with_place(
        functools.partial(query_kernel, 0),
        shapes((rows, width), BF16),
        (place, target, target_gain, query_gain),
        [(part, 0, head) for part in first],
        200000000,
    )
    chip = jnp.concatenate([queries, shifted(queries, "c", 1)], axis=0)
    everyone = [chip] + [shifted(chip, "x", k) for k in range(1, lax.axis_size("x"))]

    hidden = target
    for layer in range(layers):
        partial = with_place(
            functools.partial(attention_kernel, heads, head, 512, len(everyone)),
            shapes((group, wide), BF16),
            (place, *everyone),
            [(plane, layer, 1)],
            5000000000,
            scratch=[
                pltpu.VMEM((heads, 2 * head, group), BF16),
                pltpu.VMEM((2 * head, keys), BF16),
                pltpu.VMEM((wide, group), F32),
            ],
        )
        arrived = lax.all_to_all(partial.reshape(-1, rows, wide), TP, split_axis=0, concat_axis=0, tiled=True)
        if layer + 1 < layers:
            hidden, queries = with_place(
                functools.partial(middle_kernel, layer + 1, heads),
                [shapes((rows, model), BF16), shapes((rows, width), BF16)],
                (place, arrived, hidden, target_gain, query_gain),
                rest[0] + rest[1],
                400000000,
            )
            everyone = [to_all(queries, TP).reshape(group, width)]
        else:
            hidden = with_place(
                functools.partial(last_kernel, heads, head),
                shapes((rows, model), BF16),
                (place, arrived, hidden),
                rest[2],
                200000000,
            )
    return hidden


def solution(mesh):
    columns = mesh.shape["tp"]
    split = Mesh(mesh.devices.reshape(8, 8, columns // 2, 2), ALL)
    return jax.shard_map(
        decoder,
        mesh=split,
        in_specs=(P(ALL, None), P(ALL, None), P(), P(), P(), P(), P(None, None, TP), P(), P(), P(None, TP, None)),
        out_specs=P(ALL, None),
        check_vma=False,
    )
```

```python
import functools

import jax
import jax.numpy as jnp
from jax import lax
from jax.experimental import pallas as pl
from jax.experimental.pallas import tpu as pltpu
from jax.sharding import Mesh
from jax.sharding import PartitionSpec as P

ROWS = ("z", "y")
TP = ("x", "c")
ALL = ("z", "y", "x", "c")
EPS = 1e-06
LOG2E = 1.4426950408889634
F32 = jnp.float32
BF16 = jnp.bfloat16


def dot(a, b):
    return jnp.dot(a, b, preferred_element_type=F32)


def dot_t(a, b):
    return lax.dot_general(a, b, (((1,), (1,)), ((), ())), preferred_element_type=F32)


def rms(value):
    return lax.rsqrt(jnp.mean(value * value, axis=-1, keepdims=True) + EPS)


def head_norm(value, gain_row, head):
    rows, width = value.shape
    low = lax.broadcasted_iota(jnp.int32, (rows, 2 * head), 1) < head
    groups = []
    for start in range(0, width, 2 * head):
        part = value[:, start : start + 2 * head]
        square = part * part
        first = jnp.sum(jnp.where(low, square, 0.0), axis=-1, keepdims=True)
        second = jnp.sum(jnp.where(low, 0.0, square), axis=-1, keepdims=True)
        scale = lax.rsqrt(jnp.where(low, first, second) / head + EPS)
        groups.append(part * scale * gain_row)
    return groups


def doubled(row):
    return jnp.concatenate([row, row], axis=-1)


def source_kernel(source, gain, key_gain, key_weight, value_weight, out):
    layers, head = key_gain.shape
    value = source[...].astype(F32)
    scaled = value * rms(value)
    width = key_weight.shape[2]
    for layer in range(layers):
        normed = (scaled * gain[layer : layer + 1, :]).astype(BF16)
        keys = dot(normed, key_weight[layer])
        row = doubled(key_gain[layer : layer + 1, :])
        groups = head_norm(keys, row, head)
        for k, group in enumerate(groups):
            out[layer, :, k * 2 * head : (k + 1) * 2 * head] = group.astype(BF16)
        out[layer, :, width:] = dot(normed, value_weight[layer]).astype(BF16)


def project(normed, mine, other, row, head, place):
    x, core = place[0], place[1]
    model = normed.shape[1]
    own = jnp.concatenate(head_norm(dot_t(normed, mine.reshape(-1, model)), row, head), axis=1)
    far = jnp.concatenate(head_norm(dot_t(normed, other.reshape(-1, model)), row, head), axis=1)
    own = pltpu.roll(own, x * head, 1)
    far = pltpu.roll(far, x * head, 1)
    return jnp.where(core == 0, own, far), jnp.where(core == 0, far, own)


def store_groups(out, groups):
    width = groups[0].shape[1]
    for k, group in enumerate(groups):
        out[:, k * width : (k + 1) * width] = group.astype(BF16)


def query_kernel(layer, place, target, beside, gain, query_gain, mine, other, out):
    head = query_gain.shape[1]
    value = jnp.concatenate([target[...].astype(F32), beside[...].astype(F32)], axis=0)
    normed = (value * rms(value) * gain[layer : layer + 1, :]).astype(BF16)
    row = doubled(query_gain[layer : layer + 1, :])
    store_groups(out, project(normed, mine[...], other[...], row, head, place))


def attended_halves(arrived, heads, head):
    total = arrived[0].astype(F32)
    for k in range(1, arrived.shape[0]):
        total = total + arrived[k].astype(F32)
    rows = total.shape[0]
    width = heads * head
    mass = total[:, width : width + heads] + total[:, width + heads : width + 2 * heads]
    low = lax.broadcasted_iota(jnp.int32, (rows, 2 * head), 1) < head
    groups = []
    for g in range(heads // 2):
        below = jnp.where(low, mass[:, 2 * g : 2 * g + 1], mass[:, 2 * g + 1 : 2 * g + 2])
        groups.append(total[:, 2 * g * head : 2 * (g + 1) * head] / below)
    half = len(groups) // 2
    return jnp.concatenate(groups[:half], axis=1), jnp.concatenate(groups[half:], axis=1)


def mixed(place, arrived, hidden, mine, other, heads, head):
    x, core = place[0], place[1]
    even, odd = attended_halves(arrived, heads, head)
    width = even.shape[1]
    back = (width - x * head) % width
    own = pltpu.roll(jnp.where(core == 0, even, odd), back, 1).astype(BF16)
    far = pltpu.roll(jnp.where(core == 0, odd, even), back, 1).astype(BF16)
    model = hidden.shape[1]
    branch = dot(own, mine[...].reshape(-1, model)) + dot(far, other[...].reshape(-1, model))
    return (hidden[...].astype(F32) + branch).astype(BF16)


def middle_kernel(layer, heads, place, arrived, hidden, gain, query_gain, out_mine, out_other, mine, other, hidden_out, out):
    head = query_gain.shape[1]
    now = mixed(place, arrived, hidden, out_mine, out_other, heads, head)
    hidden_out[...] = now
    value = now.astype(F32)
    normed = (value * rms(value) * gain[layer : layer + 1, :]).astype(BF16)
    row = doubled(query_gain[layer : layer + 1, :])
    store_groups(out, project(normed, mine[...], other[...], row, head, place))


def last_kernel(heads, head, place, arrived, hidden, out_mine, out_other, hidden_out):
    hidden_out[...] = mixed(place, arrived, hidden, out_mine, out_other, heads, head)


def attention_kernel(heads, head, tile, count, place, *refs):
    queries, (pairs, out, rhs, value_t, gathered) = refs[:count], refs[count:]
    blocks, each_rows, _ = pairs.shape
    keys = blocks * each_rows
    width = 2 * head
    everyone = jnp.concatenate([part[...].astype(F32) for part in queries], axis=0)
    columns = everyone.shape[0]
    factor = LOG2E * head**-0.5
    turned = jnp.transpose(everyone).astype(BF16)
    zero = jnp.zeros((head, columns), BF16)
    per = heads // 4
    for p in range(heads):
        kv = (p % 4) // 2
        rhs[p, kv * head : (kv + 1) * head, :] = turned[p * head : (p + 1) * head, :]
        rhs[p, (1 - kv) * head : (2 - kv) * head, :] = zero
    value_t[...] = jnp.transpose(pairs[:, :, width:].reshape(keys, width).astype(F32)).astype(BF16)
    for kv in range(2):

        def one_head(j, carry, kv=kv):
            p = (j // 2) * 4 + 2 * kv + j % 2
            right = rhs[p]
            mass = jnp.zeros((8, columns), F32)
            total = None
            for t in range(keys // tile):
                taken = slice(t * tile // each_rows, (t + 1) * tile // each_rows)
                score = dot(pairs[taken, :, :width].reshape(tile, width), right)
                weight = jnp.exp2(score * factor)
                mass = mass + jnp.sum(weight.reshape(tile // 8, 8, columns), axis=0)
                part = dot(value_t[:, t * tile : (t + 1) * tile], weight.astype(BF16))
                total = part if total is None else total + part
            gathered[pl.ds(pl.multiple_of(p * head, head), head), :] = total[kv * head : (kv + 1) * head, :]
            mass = jnp.sum(mass, axis=0, keepdims=True)
            top = mass.astype(BF16).astype(F32)
            gathered[pl.ds(heads * head + p, 1), :] = top
            gathered[pl.ds(heads * head + heads + p, 1), :] = mass - top
            return carry

        lax.fori_loop(0, 2 * per, one_head, 0, unroll=True)
    rest = heads * head + 2 * heads
    gathered[rest:, :] = jnp.zeros((gathered.shape[0] - rest, columns), F32)
    result = jnp.transpose(gathered[...]).astype(BF16)
    if count == 1:
        out[...] = result
        return
    each = columns // (2 * count)
    for r in range(count):
        for d in range(2):
            to = ((place[0] + r) % count) * 2 + (place[1] + d) % 2
            first = (2 * r + d) * each
            out[pl.ds(pl.multiple_of(to * each, each), each), :] = result[first : first + each, :]


def whole(value):
    return pl.BlockSpec(value.shape, lambda i, n=value.ndim: (0,) * n)


def part_of(value, k, size):
    if value.ndim == 4:
        return pl.BlockSpec((value.shape[0], None, *value.shape[2:]), lambda i, k=k: (0, k, 0, 0))
    return pl.BlockSpec((value.shape[0], size, value.shape[2]), lambda i, k=k: (0, k, 0))


def with_place(kernel, shapes, operands, parts, flops, scratch=(), limit=40):
    one = not isinstance(shapes, (list, tuple))
    place, *rest = operands
    placed = [] if place is None else [place]
    specs = [pl.BlockSpec(memory_space=pltpu.SMEM)] * len(placed) + [whole(value) for value in rest]
    specs += [part_of(*part) for part in parts]
    return pl.pallas_call(
        kernel,
        grid=(1,),
        out_shape=shapes,
        in_specs=specs,
        out_specs=whole(shapes) if one else [whole(shape) for shape in shapes],
        scratch_shapes=list(scratch),
        compiler_params=pltpu.CompilerParams(vmem_limit_bytes=limit * 1024 * 1024),
        cost_estimate=pl.CostEstimate(flops=flops, bytes_accessed=1000000, transcendentals=0),
    )(*placed, *rest, *(part[0] for part in parts))


def to_all(value, axis):
    copies = jnp.broadcast_to(value, (lax.axis_size(axis), *value.shape))
    return lax.all_to_all(copies, axis, split_axis=0, concat_axis=0, tiled=True)


def shifted(value, axis, step):
    size = lax.axis_size(axis)
    return lax.ppermute(value, axis, [((k + step) % size, k) for k in range(size)])


def around(value):
    half = value.shape[0] // 2
    right, left = shifted(value, "x", 1), shifted(value, "x", -1)
    far = [shifted(right[:half], "x", 1), shifted(left[half:], "x", -1)]
    return [value, right, *far, left]


def decoder(target, source, target_gain, source_gain, query_gain, key_gain, query_weight, key_weight, value_weight, out_weight):
    layers, _, head_columns = query_weight.shape
    head = query_gain.shape[1]
    heads = head_columns // head * lax.axis_size(TP)
    rows, model = target.shape
    group = rows * lax.axis_size(TP)
    shapes = jax.ShapeDtypeStruct
    place = jnp.stack([lax.axis_index("x"), lax.axis_index("c")])
    query_t = jnp.swapaxes(query_weight, 1, 2)
    width = heads * head
    wide = width + 128

    pairs = with_place(
        source_kernel,
        shapes((layers, rows, 4 * head), BF16),
        (None, source, source_gain, key_gain, key_weight, value_weight),
        [],
        200000000,
        limit=63,
    )
    plane = to_all(pairs, ROWS)
    keys = plane.shape[0] * rows

    def both(stacked):
        return stacked, shifted(stacked, "c", 1)

    beside = [query_t[0]] + [shifted(query_t[0], "x", k) for k in range(1, lax.axis_size("x"))]
    first = both(jnp.stack(beside))
    pieces = around(jnp.concatenate([out_weight[0], query_t[1], out_weight[1]], axis=0))

    chip = with_place(
        functools.partial(query_kernel, 0),
        shapes((2 * rows, width), BF16),
        (place, target, shifted(target, "c", 1), target_gain, query_gain),
        [(part, 0, head) for part in first],
        200000000,
    )
    everyone = [chip] + [shifted(chip, "x", k) for k in range(1, lax.axis_size("x"))]

    hidden = target
    for layer in range(layers):
        partial = with_place(
            functools.partial(attention_kernel, heads, head, 512, len(everyone)),
            shapes((group, wide), BF16),
            (place, *everyone),
            [(plane, layer, 1)],
            5000000000,
            scratch=[
                pltpu.VMEM((heads, 2 * head, group), BF16),
                pltpu.VMEM((2 * head, keys), BF16),
                pltpu.VMEM((wide, group), F32),
            ],
        )
        if layer == 0:
            pieces, _ = lax.optimization_barrier((pieces, partial))
            right = jnp.concatenate(pieces[2:4], axis=0)
            rest = both(jnp.stack([pieces[0], pieces[1], right, pieces[4]]))
            rest = [[(part, k, head) for part in rest] for k in range(3)]
        arrived = lax.all_to_all(partial.reshape(-1, rows, wide), TP, split_axis=0, concat_axis=0, tiled=True)
        if layer + 1 < layers:
            hidden, queries = with_place(
                functools.partial(middle_kernel, layer + 1, heads),
                [shapes((rows, model), BF16), shapes((rows, width), BF16)],
                (place, arrived, hidden, target_gain, query_gain),
                rest[0] + rest[1],
                400000000,
            )
            everyone = [to_all(queries, TP).reshape(group, width)]
        else:
            hidden = with_place(
                functools.partial(last_kernel, heads, head),
                shapes((rows, model), BF16),
                (place, arrived, hidden),
                rest[2],
                200000000,
            )
    return hidden


def solution(mesh):
    columns = mesh.shape["tp"]
    split = Mesh(mesh.devices.reshape(8, 8, columns // 2, 2), ALL)
    return jax.shard_map(
        decoder,
        mesh=split,
        in_specs=(P(ALL, None), P(ALL, None), P(), P(), P(), P(), P(None, None, TP), P(), P(), P(None, TP, None)),
        out_specs=P(ALL, None),
        check_vma=False,
    )
```

```python
import functools

import jax
import jax.numpy as jnp
from jax import lax
from jax.experimental import pallas as pl
from jax.experimental.pallas import tpu as pltpu
from jax.sharding import Mesh
from jax.sharding import PartitionSpec as P

ROWS = ("z", "y")
TP = ("x", "c")
ALL = ("z", "y", "x", "c")
EPS = 1e-06
LOG2E = 1.4426950408889634
F32 = jnp.float32
BF16 = jnp.bfloat16


def dot(a, b):
    return jnp.dot(a, b, preferred_element_type=F32)


def dot_t(a, b):
    return lax.dot_general(a, b, (((1,), (1,)), ((), ())), preferred_element_type=F32)


def rms(value):
    return lax.rsqrt(jnp.mean(value * value, axis=-1, keepdims=True) + EPS)


def head_norm(value, gain_row, head):
    rows, width = value.shape
    low = lax.broadcasted_iota(jnp.int32, (rows, 2 * head), 1) < head
    groups = []
    for start in range(0, width, 2 * head):
        part = value[:, start : start + 2 * head]
        square = part * part
        first = jnp.sum(jnp.where(low, square, 0.0), axis=-1, keepdims=True)
        second = jnp.sum(jnp.where(low, 0.0, square), axis=-1, keepdims=True)
        scale = lax.rsqrt(jnp.where(low, first, second) / head + EPS)
        groups.append(part * scale * gain_row)
    return groups


def doubled(row):
    return jnp.concatenate([row, row], axis=-1)


def source_kernel(source, gain, key_gain, key_weight, value_weight, out):
    layers, head = key_gain.shape
    value = source[...].astype(F32)
    scaled = value * rms(value)
    width = key_weight.shape[2]
    for layer in range(layers):
        normed = (scaled * gain[layer : layer + 1, :]).astype(BF16)
        keys = dot(normed, key_weight[layer])
        row = doubled(key_gain[layer : layer + 1, :])
        groups = head_norm(keys, row, head)
        for k, group in enumerate(groups):
            out[layer, :, k * 2 * head : (k + 1) * 2 * head] = group.astype(BF16)
        out[layer, :, width:] = dot(normed, value_weight[layer]).astype(BF16)


def project(normed, mine, other, row, head, place):
    x, core = place[0], place[1]
    model = normed.shape[1]
    own = jnp.concatenate(head_norm(dot_t(normed, mine.reshape(-1, model)), row, head), axis=1)
    far = jnp.concatenate(head_norm(dot_t(normed, other.reshape(-1, model)), row, head), axis=1)
    own = pltpu.roll(own, x * head, 1)
    far = pltpu.roll(far, x * head, 1)
    return jnp.where(core == 0, own, far), jnp.where(core == 0, far, own)


def store_groups(out, groups):
    width = groups[0].shape[1]
    for k, group in enumerate(groups):
        out[:, k * width : (k + 1) * width] = group.astype(BF16)


def query_kernel(layer, place, target, beside, gain, query_gain, mine, other, out):
    head = query_gain.shape[1]
    value = jnp.concatenate([target[...].astype(F32), beside[...].astype(F32)], axis=0)
    normed = (value * rms(value) * gain[layer : layer + 1, :]).astype(BF16)
    row = doubled(query_gain[layer : layer + 1, :])
    store_groups(out, project(normed, mine[...], other[...], row, head, place))


def attended_halves(arrived, heads, head):
    total = arrived[0].astype(F32)
    for k in range(1, arrived.shape[0]):
        total = total + arrived[k].astype(F32)
    rows = total.shape[0]
    width = heads * head
    mass = total[:, width : width + heads] + total[:, width + heads : width + 2 * heads]
    low = lax.broadcasted_iota(jnp.int32, (rows, 2 * head), 1) < head
    groups = []
    for g in range(heads // 2):
        below = jnp.where(low, mass[:, 2 * g : 2 * g + 1], mass[:, 2 * g + 1 : 2 * g + 2])
        groups.append(total[:, 2 * g * head : 2 * (g + 1) * head] / below)
    half = len(groups) // 2
    return jnp.concatenate(groups[:half], axis=1), jnp.concatenate(groups[half:], axis=1)


def mixed(place, arrived, hidden, mine, other, heads, head):
    x, core = place[0], place[1]
    even, odd = attended_halves(arrived, heads, head)
    width = even.shape[1]
    back = (width - x * head) % width
    own = pltpu.roll(jnp.where(core == 0, even, odd), back, 1).astype(BF16)
    far = pltpu.roll(jnp.where(core == 0, odd, even), back, 1).astype(BF16)
    model = hidden.shape[1]
    branch = dot(own, mine[...].reshape(-1, model)) + dot(far, other[...].reshape(-1, model))
    return (hidden[...].astype(F32) + branch).astype(BF16)


def middle_kernel(layer, heads, place, arrived, hidden, gain, query_gain, out_mine, out_other, mine, other, hidden_out, out):
    head = query_gain.shape[1]
    now = mixed(place, arrived, hidden, out_mine, out_other, heads, head)
    hidden_out[...] = now
    value = now.astype(F32)
    normed = (value * rms(value) * gain[layer : layer + 1, :]).astype(BF16)
    row = doubled(query_gain[layer : layer + 1, :])
    store_groups(out, project(normed, mine[...], other[...], row, head, place))


def last_kernel(heads, head, place, arrived, hidden, out_mine, out_other, hidden_out):
    hidden_out[...] = mixed(place, arrived, hidden, out_mine, out_other, heads, head)


def attention_kernel(heads, head, tile, counts, place, *refs):
    count, shards = counts
    queries, planes, (out, rhs, value_t, gathered) = refs[:count], refs[count : count + shards], refs[count + shards :]
    blocks, each_rows, _ = planes[0].shape
    shard = blocks * each_rows
    width = 2 * head
    everyone = jnp.concatenate([part[...].astype(F32).reshape(-1, heads * head) for part in queries], axis=0)
    rows = everyone.shape[0]
    groups, _, columns = rhs.shape
    pack = columns // rows
    factor = LOG2E * head**-0.5
    turned = jnp.transpose(everyone).astype(BF16)
    zero = jnp.zeros((head, columns), BF16)

    def key_head(group):
        return group * pack % 4 // 2

    for group in range(groups):
        kv = key_head(group)
        for k in range(pack):
            p = group * pack + k
            rhs[group, kv * head : (kv + 1) * head, k * rows : (k + 1) * rows] = turned[p * head : (p + 1) * head, :]
        rhs[group, (1 - kv) * head : (2 - kv) * head, :] = zero
    for n, pairs in enumerate(planes):
        flat = pairs[:, :, width:].reshape(shard, width).astype(F32)
        value_t[:, n * shard : (n + 1) * shard] = jnp.transpose(flat).astype(BF16)
    for group in range(groups):
        kv = key_head(group)
        right = rhs[group]
        mass = jnp.zeros((8, columns), F32)
        total = None
        for n, pairs in enumerate(planes):
            for t in range(shard // tile):
                taken = slice(t * tile // each_rows, (t + 1) * tile // each_rows)
                score = dot(pairs[taken, :, :width].reshape(tile, width), right)
                weight = jnp.exp2(score * factor)
                mass = mass + jnp.sum(weight.reshape(tile // 8, 8, columns), axis=0)
                first = n * shard + t * tile
                part = dot(value_t[:, first : first + tile], weight.astype(BF16))
                total = part if total is None else total + part
        mass = jnp.sum(mass, axis=0, keepdims=True)
        top = mass.astype(BF16).astype(F32)
        for k in range(pack):
            p = group * pack + k
            here = slice(k * rows, (k + 1) * rows)
            gathered[p * head : (p + 1) * head, :] = total[kv * head : (kv + 1) * head, here]
            gathered[heads * head + p : heads * head + p + 1, :] = top[:, here]
            gathered[heads * head + heads + p : heads * head + heads + p + 1, :] = (mass - top)[:, here]
    rest = heads * head + 2 * heads
    gathered[rest:, :] = jnp.zeros((gathered.shape[0] - rest, rows), F32)
    result = jnp.transpose(gathered[...]).astype(BF16)
    if count == 1:
        out[...] = result
        return
    each = rows // (2 * count)
    for r in range(count):
        for d in range(2):
            to = ((place[0] + r) % count) * 2 + (place[1] + d) % 2
            first = (2 * r + d) * each
            out[pl.ds(pl.multiple_of(to * each, each), each), :] = result[first : first + each, :]


def whole(value):
    return pl.BlockSpec(value.shape, lambda i, n=value.ndim: (0,) * n)


def part_of(value, k, size):
    if value.ndim == 4:
        return pl.BlockSpec((value.shape[0], None, *value.shape[2:]), lambda i, k=k: (0, k, 0, 0))
    return pl.BlockSpec((value.shape[0], size, value.shape[2]), lambda i, k=k: (0, k, 0))


def with_place(kernel, shapes, operands, parts, flops, scratch=(), limit=24):
    one = not isinstance(shapes, (list, tuple))
    place, *rest = operands
    placed = [] if place is None else [place]
    specs = [pl.BlockSpec(memory_space=pltpu.SMEM)] * len(placed) + [whole(value) for value in rest]
    specs += [part_of(*part) for part in parts]
    return pl.pallas_call(
        kernel,
        grid=(1,),
        out_shape=shapes,
        in_specs=specs,
        out_specs=whole(shapes) if one else [whole(shape) for shape in shapes],
        scratch_shapes=list(scratch),
        compiler_params=pltpu.CompilerParams(vmem_limit_bytes=limit * 1024 * 1024),
        cost_estimate=pl.CostEstimate(flops=flops, bytes_accessed=1000000, transcendentals=0),
    )(*placed, *rest, *(part[0] for part in parts))


def to_all(value, axis):
    copies = jnp.broadcast_to(value, (lax.axis_size(axis), *value.shape))
    return lax.all_to_all(copies, axis, split_axis=0, concat_axis=0, tiled=True)


def shifted(value, axis, step):
    size = lax.axis_size(axis)
    return lax.ppermute(value, axis, [((k + step) % size, k) for k in range(size)])


def around(value):
    half = value.shape[0] // 2
    right, left = shifted(value, "x", 1), shifted(value, "x", -1)
    far = [shifted(right[:half], "x", 1), shifted(left[half:], "x", -1)]
    return [value, right, *far, left]


def decoder(target, source, target_gain, source_gain, query_gain, key_gain, query_weight, key_weight, value_weight, out_weight):
    layers, _, head_columns = query_weight.shape
    head = query_gain.shape[1]
    heads = head_columns // head * lax.axis_size(TP)
    rows, model = target.shape
    group = rows * lax.axis_size(TP)
    shapes = jax.ShapeDtypeStruct
    place = jnp.stack([lax.axis_index("x"), lax.axis_index("c")])
    query_t = jnp.swapaxes(query_weight, 1, 2)
    width = heads * head
    wide = width + 128

    pairs = with_place(
        source_kernel,
        shapes((layers, rows, 4 * head), BF16),
        (None, source, source_gain, key_gain, key_weight, value_weight),
        [],
        200000000,
        limit=63,
    )
    plane = to_all(pairs, ROWS)
    keys = plane.shape[0] * rows

    def both(stacked):
        return stacked, shifted(stacked, "c", 1)

    beside = [query_t[0]] + [shifted(query_t[0], "x", k) for k in range(1, lax.axis_size("x"))]
    first = both(jnp.stack(beside))
    pieces = around(jnp.concatenate([out_weight[0], query_t[1], out_weight[1]], axis=0))

    chip = with_place(
        functools.partial(query_kernel, 0),
        shapes((2 * rows, width), BF16),
        (place, target, shifted(target, "c", 1), target_gain, query_gain),
        [(part, 0, head) for part in first],
        200000000,
    )
    everyone = [chip] + [shifted(chip, "x", k) for k in range(1, lax.axis_size("x"))]

    def attend(everyone, parts, members):
        columns = group
        return with_place(
            functools.partial(attention_kernel, heads, head, 512, (len(everyone), len(parts))),
            shapes((members * rows, wide), BF16),
            (place, *everyone),
            parts,
            5000000000,
            scratch=[
                pltpu.VMEM((heads * members * rows // columns, 2 * head, columns), BF16),
                pltpu.VMEM((2 * head, len(parts) * keys), BF16),
                pltpu.VMEM((wide, members * rows), F32),
            ],
            limit=52,
        )

    def returned(partial, axis):
        return lax.all_to_all(partial.reshape(-1, rows, wide), axis, split_axis=0, concat_axis=0, tiled=True)

    partial = attend(everyone, [(plane, 0, 1)], lax.axis_size(TP))
    pieces, second, _ = lax.optimization_barrier((pieces, plane, partial))
    far = jnp.concatenate(pieces[2:4], axis=0)
    rest = both(jnp.stack([pieces[0], pieces[1], far, pieces[4]]))
    rest = [[(part, k, head) for part in rest] for k in range(3)]
    shared = shifted(second[:, 1:2], "c", 1)
    arrived = returned(partial, TP)
    hidden, queries = with_place(
        functools.partial(middle_kernel, 1, heads),
        [shapes((rows, model), BF16), shapes((rows, width), BF16)],
        (place, arrived, target, target_gain, query_gain),
        rest[0] + rest[1],
        400000000,
    )
    partial = attend([to_all(queries, "x")], [(plane, 1, 1), (shared, 0, 1)], lax.axis_size("x"))
    return with_place(
        functools.partial(last_kernel, heads, head),
        shapes((rows, model), BF16),
        (place, returned(partial, "x"), hidden),
        rest[2],
        200000000,
    )


def solution(mesh):
    columns = mesh.shape["tp"]
    split = Mesh(mesh.devices.reshape(8, 8, columns // 2, 2), ALL)
    return jax.shard_map(
        decoder,
        mesh=split,
        in_specs=(P(ALL, None), P(ALL, None), P(), P(), P(), P(), P(None, None, TP), P(), P(), P(None, TP, None)),
        out_specs=P(ALL, None),
        check_vma=False,
    )
```

```python
import functools

import jax
import jax.numpy as jnp
from jax import lax
from jax.experimental import pallas as pl
from jax.experimental.pallas import tpu as pltpu
from jax.sharding import Mesh
from jax.sharding import PartitionSpec as P

ROWS = ("z", "y")
TP = ("x", "c")
ALL = ("z", "y", "x", "c")
EPS = 1e-06
LOG2E = 1.4426950408889634
F32 = jnp.float32
BF16 = jnp.bfloat16


def dot(a, b):
    return jnp.dot(a, b, preferred_element_type=F32)


def dot_t(a, b):
    return lax.dot_general(a, b, (((1,), (1,)), ((), ())), preferred_element_type=F32)


def rms(value):
    return lax.rsqrt(jnp.mean(value * value, axis=-1, keepdims=True) + EPS)


def head_norm(value, gain_row, head):
    rows, width = value.shape
    low = lax.broadcasted_iota(jnp.int32, (rows, 2 * head), 1) < head
    groups = []
    for start in range(0, width, 2 * head):
        part = value[:, start : start + 2 * head]
        square = part * part
        first = jnp.sum(jnp.where(low, square, 0.0), axis=-1, keepdims=True)
        second = jnp.sum(jnp.where(low, 0.0, square), axis=-1, keepdims=True)
        scale = lax.rsqrt(jnp.where(low, first, second) / head + EPS)
        groups.append(part * scale * gain_row)
    return groups


def doubled(row):
    return jnp.concatenate([row, row], axis=-1)


def source_kernel(source, gain, key_gain, key_weight, value_weight, out):
    layers, head = key_gain.shape
    value = source[...].astype(F32)
    scaled = value * rms(value)
    width = key_weight.shape[2]
    for layer in range(layers):
        normed = (scaled * gain[layer : layer + 1, :]).astype(BF16)
        keys = dot(normed, key_weight[layer])
        row = doubled(key_gain[layer : layer + 1, :])
        groups = head_norm(keys, row, head)
        for k, group in enumerate(groups):
            out[0, layer, :, k * 2 * head : (k + 1) * 2 * head] = group.astype(BF16)
        out[0, layer, :, width:] = dot(normed, value_weight[layer]).astype(BF16)
    result = out[0]
    for k in range(1, out.shape[0]):
        out[k] = result


def project(normed, mine, other, row, head, place):
    x, core = place[0], place[1]
    model = normed.shape[1]
    own = jnp.concatenate(head_norm(dot_t(normed, mine.reshape(-1, model)), row, head), axis=1)
    far = jnp.concatenate(head_norm(dot_t(normed, other.reshape(-1, model)), row, head), axis=1)
    own = pltpu.roll(own, x * head, 1)
    far = pltpu.roll(far, x * head, 1)
    return jnp.where(core == 0, own, far), jnp.where(core == 0, far, own)


def store_groups(out, groups):
    width = groups[0].shape[1]
    for k, group in enumerate(groups):
        out[:, k * width : (k + 1) * width] = group.astype(BF16)


def query_kernel(layer, place, target, beside, gain, query_gain, mine, other, out):
    head = query_gain.shape[1]
    value = jnp.concatenate([target[...].astype(F32), beside[...].astype(F32)], axis=0)
    normed = (value * rms(value) * gain[layer : layer + 1, :]).astype(BF16)
    row = doubled(query_gain[layer : layer + 1, :])
    store_groups(out, project(normed, mine[...], other[...], row, head, place))


def attended_halves(arrived, heads, head):
    total = arrived[0].astype(F32)
    for k in range(1, arrived.shape[0]):
        total = total + arrived[k].astype(F32)
    rows = total.shape[0]
    width = heads * head
    mass = total[:, width : width + heads] + total[:, width + heads : width + 2 * heads]
    low = lax.broadcasted_iota(jnp.int32, (rows, 2 * head), 1) < head
    groups = []
    for g in range(heads // 2):
        below = jnp.where(low, mass[:, 2 * g : 2 * g + 1], mass[:, 2 * g + 1 : 2 * g + 2])
        groups.append(total[:, 2 * g * head : 2 * (g + 1) * head] / below)
    half = len(groups) // 2
    return jnp.concatenate(groups[:half], axis=1), jnp.concatenate(groups[half:], axis=1)


def mixed(place, arrived, hidden, mine, other, heads, head):
    x, core = place[0], place[1]
    even, odd = attended_halves(arrived, heads, head)
    width = even.shape[1]
    back = (width - x * head) % width
    own = pltpu.roll(jnp.where(core == 0, even, odd), back, 1).astype(BF16)
    far = pltpu.roll(jnp.where(core == 0, odd, even), back, 1).astype(BF16)
    model = hidden.shape[1]
    branch = dot(own, mine[...].reshape(-1, model)) + dot(far, other[...].reshape(-1, model))
    return (hidden[...].astype(F32) + branch).astype(BF16)


def middle_kernel(layer, heads, place, arrived, hidden, gain, query_gain, out_mine, out_other, mine, other, hidden_out, out):
    head = query_gain.shape[1]
    now = mixed(place, arrived, hidden, out_mine, out_other, heads, head)
    hidden_out[...] = now
    value = now.astype(F32)
    normed = (value * rms(value) * gain[layer : layer + 1, :]).astype(BF16)
    row = doubled(query_gain[layer : layer + 1, :])
    halves = project(normed, mine[...], other[...], row, head, place)
    for copy in range(out.shape[0]):
        store_groups(out.at[copy], halves)


def last_kernel(heads, head, place, arrived, hidden, out_mine, out_other, hidden_out):
    hidden_out[...] = mixed(place, arrived, hidden, out_mine, out_other, heads, head)


def attention_kernel(heads, head, tile, counts, place, *refs):
    count, shards = counts
    queries, planes, (out, rhs, value_t, gathered) = refs[:count], refs[count : count + shards], refs[count + shards :]
    blocks, each_rows, _ = planes[0].shape
    shard = blocks * each_rows
    width = 2 * head
    everyone = jnp.concatenate([part[...].astype(F32).reshape(-1, heads * head) for part in queries], axis=0)
    rows = everyone.shape[0]
    groups, _, columns = rhs.shape
    pack = columns // rows
    factor = LOG2E * head**-0.5
    turned = jnp.transpose(everyone).astype(BF16)
    zero = jnp.zeros((head, columns), BF16)

    def key_head(group):
        return group * pack % 4 // 2

    for group in range(groups):
        kv = key_head(group)
        for k in range(pack):
            p = group * pack + k
            rhs[group, kv * head : (kv + 1) * head, k * rows : (k + 1) * rows] = turned[p * head : (p + 1) * head, :]
        rhs[group, (1 - kv) * head : (2 - kv) * head, :] = zero
    for n, pairs in enumerate(planes):
        flat = pairs[:, :, width:].reshape(shard, width).astype(F32)
        value_t[:, n * shard : (n + 1) * shard] = jnp.transpose(flat).astype(BF16)
    for group in range(groups):
        kv = key_head(group)
        right = rhs[group]
        mass = jnp.zeros((8, columns), F32)
        total = None
        for n, pairs in enumerate(planes):
            for t in range(shard // tile):
                taken = slice(t * tile // each_rows, (t + 1) * tile // each_rows)
                score = dot(pairs[taken, :, :width].reshape(tile, width), right)
                weight = jnp.exp2(score * factor)
                mass = mass + jnp.sum(weight.reshape(tile // 8, 8, columns), axis=0)
                first = n * shard + t * tile
                part = dot(value_t[:, first : first + tile], weight.astype(BF16))
                total = part if total is None else total + part
        mass = jnp.sum(mass, axis=0, keepdims=True)
        top = mass.astype(BF16).astype(F32)
        for k in range(pack):
            p = group * pack + k
            here = slice(k * rows, (k + 1) * rows)
            gathered[p * head : (p + 1) * head, :] = total[kv * head : (kv + 1) * head, here]
            gathered[heads * head + p : heads * head + p + 1, :] = top[:, here]
            gathered[heads * head + heads + p : heads * head + heads + p + 1, :] = (mass - top)[:, here]
    rest = heads * head + 2 * heads
    gathered[rest:, :] = jnp.zeros((gathered.shape[0] - rest, rows), F32)
    result = jnp.transpose(gathered[...]).astype(BF16)
    if count == 1:
        out[...] = result
        return
    each = rows // (2 * count)
    for r in range(count):
        for d in range(2):
            to = ((place[0] + r) % count) * 2 + (place[1] + d) % 2
            first = (2 * r + d) * each
            out[pl.ds(pl.multiple_of(to * each, each), each), :] = result[first : first + each, :]


def whole(value):
    return pl.BlockSpec(value.shape, lambda i, n=value.ndim: (0,) * n)


def part_of(value, k, size):
    if value.ndim == 4:
        return pl.BlockSpec((value.shape[0], None, *value.shape[2:]), lambda i, k=k: (0, k, 0, 0))
    return pl.BlockSpec((value.shape[0], size, value.shape[2]), lambda i, k=k: (0, k, 0))


def with_place(kernel, shapes, operands, parts, flops, scratch=(), limit=24):
    one = not isinstance(shapes, (list, tuple))
    place, *rest = operands
    placed = [] if place is None else [place]
    specs = [pl.BlockSpec(memory_space=pltpu.SMEM)] * len(placed) + [whole(value) for value in rest]
    specs += [part_of(*part) for part in parts]
    return pl.pallas_call(
        kernel,
        grid=(1,),
        out_shape=shapes,
        in_specs=specs,
        out_specs=whole(shapes) if one else [whole(shape) for shape in shapes],
        scratch_shapes=list(scratch),
        compiler_params=pltpu.CompilerParams(vmem_limit_bytes=limit * 1024 * 1024),
        cost_estimate=pl.CostEstimate(flops=flops, bytes_accessed=1000000, transcendentals=0),
    )(*placed, *rest, *(part[0] for part in parts))


def shifted(value, axis, step):
    size = lax.axis_size(axis)
    return lax.ppermute(value, axis, [((k + step) % size, k) for k in range(size)])


def around(value):
    half = value.shape[0] // 2
    right, left = shifted(value, "x", 1), shifted(value, "x", -1)
    far = [shifted(right[:half], "x", 1), shifted(left[half:], "x", -1)]
    return [value, right, *far, left]


def decoder(target, source, target_gain, source_gain, query_gain, key_gain, query_weight, key_weight, value_weight, out_weight):
    layers, _, head_columns = query_weight.shape
    head = query_gain.shape[1]
    heads = head_columns // head * lax.axis_size(TP)
    rows, model = target.shape
    group = rows * lax.axis_size(TP)
    shapes = jax.ShapeDtypeStruct
    place = jnp.stack([lax.axis_index("x"), lax.axis_index("c")])
    query_t = jnp.swapaxes(query_weight, 1, 2)
    width = heads * head
    wide = width + 128

    pairs = with_place(
        source_kernel,
        shapes((lax.axis_size(ROWS), layers, rows, 4 * head), BF16),
        (None, source, source_gain, key_gain, key_weight, value_weight),
        [],
        200000000,
        limit=63,
    )
    plane = lax.all_to_all(pairs, ROWS, split_axis=0, concat_axis=0, tiled=True)
    keys = plane.shape[0] * rows

    def both(stacked):
        return stacked, shifted(stacked, "c", 1)

    beside = [query_t[0]] + [shifted(query_t[0], "x", k) for k in range(1, lax.axis_size("x"))]
    first = both(jnp.stack(beside))
    pieces = around(jnp.concatenate([out_weight[0], query_t[1], out_weight[1]], axis=0))

    chip = with_place(
        functools.partial(query_kernel, 0),
        shapes((2 * rows, width), BF16),
        (place, target, shifted(target, "c", 1), target_gain, query_gain),
        [(part, 0, head) for part in first],
        200000000,
    )
    everyone = [chip] + [shifted(chip, "x", k) for k in range(1, lax.axis_size("x"))]

    def attend(everyone, parts, members):
        columns = group
        return with_place(
            functools.partial(attention_kernel, heads, head, 512, (len(everyone), len(parts))),
            shapes((members * rows, wide), BF16),
            (place, *everyone),
            parts,
            5000000000,
            scratch=[
                pltpu.VMEM((heads * members * rows // columns, 2 * head, columns), BF16),
                pltpu.VMEM((2 * head, len(parts) * keys), BF16),
                pltpu.VMEM((wide, members * rows), F32),
            ],
            limit=52,
        )

    def returned(partial, axis):
        return lax.all_to_all(partial.reshape(-1, rows, wide), axis, split_axis=0, concat_axis=0, tiled=True)

    partial = attend(everyone, [(plane, 0, 1)], lax.axis_size(TP))
    pieces, second, _ = lax.optimization_barrier((pieces, plane, partial))
    far = jnp.concatenate(pieces[2:4], axis=0)
    rest = both(jnp.stack([pieces[0], pieces[1], far, pieces[4]]))
    rest = [[(part, k, head) for part in rest] for k in range(3)]
    shared = shifted(second, "c", 1)
    arrived = returned(partial, TP)
    hidden, queries = with_place(
        functools.partial(middle_kernel, 1, heads),
        [shapes((rows, model), BF16), shapes((lax.axis_size("x"), rows, width), BF16)],
        (place, arrived, target, target_gain, query_gain),
        rest[0] + rest[1],
        400000000,
        limit=56,
    )
    everyone = lax.all_to_all(queries, "x", split_axis=0, concat_axis=0, tiled=True)
    partial = attend([everyone], [(plane, 1, 1), (shared, 1, 1)], lax.axis_size("x"))
    return with_place(
        functools.partial(last_kernel, heads, head),
        shapes((rows, model), BF16),
        (place, returned(partial, "x"), hidden),
        rest[2],
        200000000,
    )


def solution(mesh):
    columns = mesh.shape["tp"]
    split = Mesh(mesh.devices.reshape(8, 8, columns // 2, 2), ALL)
    return jax.shard_map(
        decoder,
        mesh=split,
        in_specs=(P(ALL, None), P(ALL, None), P(), P(), P(), P(), P(None, None, TP), P(), P(), P(None, TP, None)),
        out_specs=P(ALL, None),
        check_vma=False,
    )
```

```python
import functools

import jax
import jax.numpy as jnp
from jax import lax
from jax.experimental import pallas as pl
from jax.experimental.pallas import tpu as pltpu
from jax.sharding import Mesh
from jax.sharding import PartitionSpec as P

ROWS = ("z", "y")
TP = ("x", "c")
ALL = ("z", "y", "x", "c")
EPS = 1e-06
LOG2E = 1.4426950408889634
F32 = jnp.float32
BF16 = jnp.bfloat16


def dot(a, b):
    return jnp.dot(a, b, preferred_element_type=F32)


def dot_t(a, b):
    return lax.dot_general(a, b, (((1,), (1,)), ((), ())), preferred_element_type=F32)


def rms(value):
    return lax.rsqrt(jnp.mean(value * value, axis=-1, keepdims=True) + EPS)


def head_norm(value, gain_row, head):
    rows, width = value.shape
    low = lax.broadcasted_iota(jnp.int32, (rows, 2 * head), 1) < head
    groups = []
    for start in range(0, width, 2 * head):
        part = value[:, start : start + 2 * head]
        square = part * part
        first = jnp.sum(jnp.where(low, square, 0.0), axis=-1, keepdims=True)
        second = jnp.sum(jnp.where(low, 0.0, square), axis=-1, keepdims=True)
        scale = lax.rsqrt(jnp.where(low, first, second) / head + EPS)
        groups.append(part * scale * gain_row)
    return groups


def doubled(row):
    return jnp.concatenate([row, row], axis=-1)


def source_kernel(source, gain, key_gain, key_weight, value_weight, out):
    layers, head = key_gain.shape
    value = source[...].astype(F32)
    scaled = value * rms(value)
    width = key_weight.shape[2]
    for layer in range(layers):
        normed = (scaled * gain[layer : layer + 1, :]).astype(BF16)
        keys = dot(normed, key_weight[layer])
        row = doubled(key_gain[layer : layer + 1, :])
        groups = head_norm(keys, row, head)
        for k, group in enumerate(groups):
            out[0, layer, :, k * 2 * head : (k + 1) * 2 * head] = group.astype(BF16)
        out[0, layer, :, width:] = dot(normed, value_weight[layer]).astype(BF16)
    result = out[0]
    for k in range(1, out.shape[0]):
        out[k] = result


def project(normed, mine, other, row, head, place):
    x, core = place[0], place[1]
    model = normed.shape[1]
    own = jnp.concatenate(head_norm(dot_t(normed, mine.reshape(-1, model)), row, head), axis=1)
    far = jnp.concatenate(head_norm(dot_t(normed, other.reshape(-1, model)), row, head), axis=1)
    own = pltpu.roll(own, x * head, 1)
    far = pltpu.roll(far, x * head, 1)
    return jnp.where(core == 0, own, far), jnp.where(core == 0, far, own)


def store_groups(out, groups):
    width = groups[0].shape[1]
    for k, group in enumerate(groups):
        out[:, k * width : (k + 1) * width] = group.astype(BF16)


def query_kernel(layer, place, target, beside, gain, query_gain, mine, other, out):
    head = query_gain.shape[1]
    value = jnp.concatenate([target[...].astype(F32), beside[...].astype(F32)], axis=0)
    normed = (value * rms(value) * gain[layer : layer + 1, :]).astype(BF16)
    row = doubled(query_gain[layer : layer + 1, :])
    store_groups(out, project(normed, mine[...], other[...], row, head, place))


def attended_halves(arrived, heads, head):
    total = arrived[0].astype(F32)
    for k in range(1, arrived.shape[0]):
        total = total + arrived[k].astype(F32)
    rows = total.shape[0]
    width = heads * head
    mass = total[:, width : width + heads] + total[:, width + heads : width + 2 * heads]
    low = lax.broadcasted_iota(jnp.int32, (rows, 2 * head), 1) < head
    groups = []
    for g in range(heads // 2):
        below = jnp.where(low, mass[:, 2 * g : 2 * g + 1], mass[:, 2 * g + 1 : 2 * g + 2])
        groups.append(total[:, 2 * g * head : 2 * (g + 1) * head] / below)
    half = len(groups) // 2
    return jnp.concatenate(groups[:half], axis=1), jnp.concatenate(groups[half:], axis=1)


def mixed(place, arrived, hidden, mine, other, heads, head):
    x, core = place[0], place[1]
    even, odd = attended_halves(arrived, heads, head)
    width = even.shape[1]
    back = (width - x * head) % width
    own = pltpu.roll(jnp.where(core == 0, even, odd), back, 1).astype(BF16)
    far = pltpu.roll(jnp.where(core == 0, odd, even), back, 1).astype(BF16)
    model = hidden.shape[1]
    branch = dot(own, mine[...].reshape(-1, model)) + dot(far, other[...].reshape(-1, model))
    return (hidden[...].astype(F32) + branch).astype(BF16)


def middle_kernel(layer, heads, place, arrived, hidden, gain, query_gain, out_mine, out_other, mine, other, hidden_out, out):
    head = query_gain.shape[1]
    now = mixed(place, arrived, hidden, out_mine, out_other, heads, head)
    hidden_out[...] = now
    value = now.astype(F32)
    normed = (value * rms(value) * gain[layer : layer + 1, :]).astype(BF16)
    row = doubled(query_gain[layer : layer + 1, :])
    halves = project(normed, mine[...], other[...], row, head, place)
    for copy in range(out.shape[0]):
        store_groups(out.at[copy], halves)


def last_kernel(heads, head, place, arrived, hidden, out_mine, out_other, hidden_out):
    hidden_out[...] = mixed(place, arrived, hidden, out_mine, out_other, heads, head)


def attention_kernel(heads, head, tile, counts, place, *refs):
    count, shards = counts
    queries, planes, (out, rhs, value_t, gathered) = refs[:count], refs[count : count + shards], refs[count + shards :]
    blocks, each_rows, _ = planes[0].shape
    shard = blocks * each_rows
    width = 2 * head
    everyone = jnp.concatenate([part[...].astype(F32).reshape(-1, heads * head) for part in queries], axis=0)
    rows = everyone.shape[0]
    groups, _, columns = rhs.shape
    pack = columns // rows
    factor = LOG2E * head**-0.5
    turned = jnp.transpose(everyone).astype(BF16)
    zero = jnp.zeros((head, columns), BF16)

    def key_head(group):
        return group * pack % 4 // 2

    for group in range(groups):
        kv = key_head(group)
        for k in range(pack):
            p = group * pack + k
            rhs[group, kv * head : (kv + 1) * head, k * rows : (k + 1) * rows] = turned[p * head : (p + 1) * head, :]
        rhs[group, (1 - kv) * head : (2 - kv) * head, :] = zero
    for n, pairs in enumerate(planes):
        flat = pairs[:, :, width:].reshape(shard, width).astype(F32)
        value_t[:, n * shard : (n + 1) * shard] = jnp.transpose(flat).astype(BF16)
    for group in range(groups):
        kv = key_head(group)
        right = rhs[group]
        mass = jnp.zeros((8, columns), F32)
        total = None
        for n, pairs in enumerate(planes):
            for t in range(shard // tile):
                taken = slice(t * tile // each_rows, (t + 1) * tile // each_rows)
                score = dot(pairs[taken, :, :width].reshape(tile, width), right)
                weight = jnp.exp2(score * factor)
                mass = mass + jnp.sum(weight.reshape(tile // 8, 8, columns), axis=0)
                first = n * shard + t * tile
                part = dot(value_t[:, first : first + tile], weight.astype(BF16))
                total = part if total is None else total + part
        mass = jnp.sum(mass, axis=0, keepdims=True)
        top = mass.astype(BF16).astype(F32)
        for k in range(pack):
            p = group * pack + k
            here = slice(k * rows, (k + 1) * rows)
            gathered[p * head : (p + 1) * head, :] = total[kv * head : (kv + 1) * head, here]
            gathered[heads * head + p : heads * head + p + 1, :] = top[:, here]
            gathered[heads * head + heads + p : heads * head + heads + p + 1, :] = (mass - top)[:, here]
    rest = heads * head + 2 * heads
    gathered[rest:, :] = jnp.zeros((gathered.shape[0] - rest, rows), F32)
    result = jnp.transpose(gathered[...]).astype(BF16)
    if count == 1:
        out[...] = result
        return
    each = rows // (2 * count)
    for r in range(count):
        for d in range(2):
            to = ((place[0] + r) % count) * 2 + (place[1] + d) % 2
            first = (2 * r + d) * each
            out[pl.ds(pl.multiple_of(to * each, each), each), :] = result[first : first + each, :]


def whole(value):
    return pl.BlockSpec(value.shape, lambda i, n=value.ndim: (0,) * n)


def part_of(value, k, size):
    if value.ndim == 4:
        return pl.BlockSpec((value.shape[0], None, *value.shape[2:]), lambda i, k=k: (0, k, 0, 0))
    return pl.BlockSpec((value.shape[0], size, value.shape[2]), lambda i, k=k: (0, k, 0))


def with_place(kernel, shapes, operands, parts, flops, scratch=(), limit=24):
    one = not isinstance(shapes, (list, tuple))
    place, *rest = operands
    placed = [] if place is None else [place]
    specs = [pl.BlockSpec(memory_space=pltpu.SMEM)] * len(placed) + [whole(value) for value in rest]
    specs += [part_of(*part) for part in parts]
    return pl.pallas_call(
        kernel,
        grid=(1,),
        out_shape=shapes,
        in_specs=specs,
        out_specs=whole(shapes) if one else [whole(shape) for shape in shapes],
        scratch_shapes=list(scratch),
        compiler_params=pltpu.CompilerParams(vmem_limit_bytes=limit * 1024 * 1024),
        cost_estimate=pl.CostEstimate(flops=flops, bytes_accessed=1000000, transcendentals=0),
    )(*placed, *rest, *(part[0] for part in parts))


def shifted(value, axis, step):
    size = lax.axis_size(axis)
    return lax.ppermute(value, axis, [((k + step) % size, k) for k in range(size)])


def around(value):
    half = value.shape[0] // 2
    right, left = shifted(value, "x", 1), shifted(value, "x", -1)
    far = [shifted(right[:half], "x", 1), shifted(left[half:], "x", -1)]
    return [value, right, *far, left]


def decoder(target, source, target_gain, source_gain, query_gain, key_gain, query_weight, key_weight, value_weight, out_weight):
    layers, _, head_columns = query_weight.shape
    head = query_gain.shape[1]
    heads = head_columns // head * lax.axis_size(TP)
    rows, model = target.shape
    group = rows * lax.axis_size(TP)
    shapes = jax.ShapeDtypeStruct
    place = jnp.stack([lax.axis_index("x"), lax.axis_index("c")])
    query_t = jnp.swapaxes(query_weight, 1, 2)
    width = heads * head
    wide = width + 128

    pairs = with_place(
        source_kernel,
        shapes((lax.axis_size(ROWS), layers, rows, 4 * head), BF16),
        (None, source, source_gain, key_gain, key_weight, value_weight),
        [],
        200000000,
        limit=63,
    )
    plane = lax.all_to_all(pairs, ROWS, split_axis=0, concat_axis=0, tiled=True)
    keys = plane.shape[0] * rows

    def both(stacked):
        return stacked, shifted(stacked, "c", 1)

    beside = [query_t[0]] + [shifted(query_t[0], "x", k) for k in range(1, lax.axis_size("x"))]
    first = both(jnp.stack(beside))
    pieces = around(jnp.concatenate([out_weight[0], query_t[1], out_weight[1]], axis=0))

    chip = with_place(
        functools.partial(query_kernel, 0),
        shapes((2 * rows, width), BF16),
        (place, target, shifted(target, "c", 1), target_gain, query_gain),
        [(part, 0, head) for part in first],
        200000000,
    )
    everyone = [chip] + [shifted(chip, "x", k) for k in range(1, lax.axis_size("x"))]

    def attend(everyone, parts, members):
        columns = group
        return with_place(
            functools.partial(attention_kernel, heads, head, 512, (len(everyone), len(parts))),
            shapes((members * rows, wide), BF16),
            (place, *everyone),
            parts,
            5000000000,
            scratch=[
                pltpu.VMEM((heads * members * rows // columns, 2 * head, columns), BF16),
                pltpu.VMEM((2 * head, len(parts) * keys), BF16),
                pltpu.VMEM((wide, members * rows), F32),
            ],
            limit=52,
        )

    def returned(partial, axis):
        return lax.all_to_all(partial.reshape(-1, rows, wide), axis, split_axis=0, concat_axis=0, tiled=True)

    partial = attend(everyone, [(plane, 0, 1)], lax.axis_size(TP))
    pieces, second, _ = lax.optimization_barrier((pieces, plane, partial))
    far = jnp.concatenate(pieces[2:4], axis=0)
    beside = [pieces[0], pieces[1], far, pieces[4]]
    near = both(jnp.stack([part[: 2 * head] for part in beside]))
    late = both(jnp.stack([part[2 * head :] for part in beside]))
    rest = [[(part, k, head) for part in near] for k in range(2)] + [[(part, 0, head) for part in late]]
    shared = shifted(second, "c", 1)
    arrived = returned(partial, TP)
    hidden, queries = with_place(
        functools.partial(middle_kernel, 1, heads),
        [shapes((rows, model), BF16), shapes((lax.axis_size("x"), rows, width), BF16)],
        (place, arrived, target, target_gain, query_gain),
        rest[0] + rest[1],
        400000000,
        limit=56,
    )
    everyone = lax.all_to_all(queries, "x", split_axis=0, concat_axis=0, tiled=True)
    partial = attend([everyone], [(plane, 1, 1), (shared, 1, 1)], lax.axis_size("x"))
    return with_place(
        functools.partial(last_kernel, heads, head),
        shapes((rows, model), BF16),
        (place, returned(partial, "x"), hidden),
        rest[2],
        200000000,
    )


def solution(mesh):
    columns = mesh.shape["tp"]
    split = Mesh(mesh.devices.reshape(8, 8, columns // 2, 2), ALL)
    return jax.shard_map(
        decoder,
        mesh=split,
        in_specs=(P(ALL, None), P(ALL, None), P(), P(), P(), P(), P(None, None, TP), P(), P(), P(None, TP, None)),
        out_specs=P(ALL, None),
        check_vma=False,
    )
```
